512 devices in a mesh: fs: 64 (over z, y), tp: 8 (over x, core).
Axes of the slice: x: 4, y: 4, z: 16, core: 2. Of those that a mesh axis runs over, the one named last changes fastest.
Arguments:
- residual_in: bfloat16 [16384, 2048], P(('fs', 'tp')), may hold values from -6 to 6
- gain_first: float32 [2048], replicated, may hold values from 0.1 to 1.9
- gain_mixer: float32 [2048], replicated, may hold values from 0.1 to 1.9
- gain_second: float32 [2048], replicated, may hold values from 0.1 to 1.9
- gate_weight: float32 [2048, 6144], P('fs', 'tp'), may hold values from -0.125 to 0.125
- gate_scale: float32 [6144], P('tp'), may hold values from 0.3 to 3
- up_weight: float32 [2048, 6144], P('fs', 'tp'), may hold values from -0.125 to 0.125
- up_scale: float32 [6144], P('tp'), may hold values from 0.3 to 3
- down_weight: float32 [6144, 2048], P('tp', 'fs'), may hold values from -0.078125 to 0.078125
- down_scale: float32 [2048], P('fs'), may hold values from 0.3 to 3
- query_weight: float32 [2048, 2048], P('fs', 'tp'), may hold values from -0.125 to 0.125
- query_scale: float32 [2048], P('tp'), may hold values from 0.3 to 3
- key_weight: float32 [2048, 2048], P('fs', 'tp'), may hold values from -0.125 to 0.125
- key_scale: float32 [2048], P('tp'), may hold values from 0.3 to 3
- value_weight: float32 [2048, 2048], P('fs', 'tp'), may hold values from -0.125 to 0.125
- value_scale: float32 [2048], P('tp'), may hold values from 0.3 to 3
- output_weight: float32 [2048, 2048], P('tp', 'fs'), may hold values from -0.125 to 0.125
- output_scale: float32 [2048], P('fs'), may hold values from 0.3 to 3
Outputs:
- residual_out: bfloat16 [16384, 2048], P(('fs', 'tp'))
The draws below stay inside these ranges and needn't reach their ends.
All inputs are finite; a program needn't handle non-finite values.
Results may differ from the reference program's by a relative error of at most 0.028.
Values may be sent and summed in bfloat16 or wider, within the bound.
No kernel may reach another device: no remote copies, remote signals or barrier semaphores. Data moves between devices by JAX's collectives and lax.ppermute only.
A program may use at most 64 MiB of HBM per device.

```python
import math
import jax
import jax.numpy as jnp
from jax import lax

D = 2048
FF = 6144
HEADS = 8
HEAD_DIM = 256
MIX_WIDTH = 2048
TOK = 256
BLOCK = 64
TOKENS = 16384
N_FS = 64
N_TP = 8


def steps_of(stream_key, dims, shards, low, top_value):
    loudness, own = 1.0, jax.random.fold_in(stream_key, 6)
    for axis_at, parts in shards:
        draws = jnp.exp(jax.random.uniform(jax.random.fold_in(own, axis_at), (parts,), jnp.float32, low / len(shards), top_value / len(shards)))
        loudness = loudness * jnp.repeat(draws, dims[axis_at] // parts).reshape([-1 if axis == axis_at else 1 for axis in range(len(dims))])
    return loudness


def centred(stream_key, extent, scale, reach, split=(), kind=jnp.bfloat16):
    entries = scale * jax.random.normal(stream_key, extent, jnp.float32)
    if split:
        entries = entries * steps_of(stream_key, extent, split, -0.22, 0.18)
    return jnp.clip(entries, -reach, reach).astype(kind)


def setup_inputs(seed: int = 0) -> dict:
    key_list = jax.random.split(jax.random.key(seed), 19)
    residual_in = centred(key_list[0], (TOKENS, D), 1.0, 6.0, ((0, 512),))
    gain_first = jnp.clip(1.0 + 0.18 * jax.random.normal(key_list[1], (D,), jnp.float32), 0.1, 1.9)
    gain_mixer = jnp.clip(1.0 + 0.18 * jax.random.normal(key_list[2], (D,), jnp.float32), 0.1, 1.9)
    gain_second = jnp.clip(1.0 + 0.18 * jax.random.normal(key_list[3], (D,), jnp.float32), 0.1, 1.9)
    gate_weight = centred(key_list[4], (D, FF), D ** -0.5, 0.125, ((0, 64), (1, 8)), jnp.float32)
    gate_scale = jnp.clip(jnp.exp(math.log(3.0) - 2.3025851 * jax.random.uniform(key_list[5], (FF,), jnp.float32) ** steps_of(key_list[5], (FF,), ((0, 8),), -0.2, 0.2)), 0.3, 3.0)
    up_weight = centred(key_list[6], (D, FF), D ** -0.5, 0.125, ((0, 64), (1, 8)), jnp.float32)
    up_scale = jnp.clip(jnp.exp(math.log(3.0) - 2.3025851 * jax.random.uniform(key_list[7], (FF,), jnp.float32) ** steps_of(key_list[7], (FF,), ((0, 8),), -0.2, 0.2)), 0.3, 3.0)
    down_weight = centred(key_list[8], (FF, D), FF ** -0.5, 0.078125, ((0, 8), (1, 64)), jnp.float32)
    down_scale = jnp.clip(jnp.exp(math.log(3.0) - 2.3025851 * jax.random.uniform(key_list[9], (D,), jnp.float32) ** steps_of(key_list[9], (D,), ((0, 64),), -0.2, 0.2)), 0.3, 3.0)
    query_weight = centred(key_list[10], (D, MIX_WIDTH), D ** -0.5, 0.125, ((0, 64), (1, 8)), jnp.float32)
    query_scale = jnp.clip(jnp.exp(math.log(3.0) - 2.3025851 * jax.random.uniform(key_list[11], (MIX_WIDTH,), jnp.float32) ** steps_of(key_list[11], (MIX_WIDTH,), ((0, 8),), -0.2, 0.2)), 0.3, 3.0)
    key_weight = centred(key_list[12], (D, MIX_WIDTH), D ** -0.5, 0.125, ((0, 64), (1, 8)), jnp.float32)
    key_scale = jnp.clip(jnp.exp(math.log(3.0) - 2.3025851 * jax.random.uniform(key_list[13], (MIX_WIDTH,), jnp.float32) ** steps_of(key_list[13], (MIX_WIDTH,), ((0, 8),), -0.2, 0.2)), 0.3, 3.0)
    value_weight = centred(key_list[14], (D, MIX_WIDTH), D ** -0.5, 0.125, ((0, 64), (1, 8)), jnp.float32)
    value_scale = jnp.clip(jnp.exp(math.log(3.0) - 2.3025851 * jax.random.uniform(key_list[15], (MIX_WIDTH,), jnp.float32) ** steps_of(key_list[15], (MIX_WIDTH,), ((0, 8),), -0.2, 0.2)), 0.3, 3.0)
    output_weight = centred(key_list[16], (MIX_WIDTH, D), MIX_WIDTH ** -0.5, 0.125, ((0, 8), (1, 64)), jnp.float32)
    output_scale = jnp.clip(jnp.exp(math.log(3.0) - 2.3025851 * jax.random.uniform(key_list[17], (D,), jnp.float32) ** steps_of(key_list[17], (D,), ((0, 64),), -0.2, 0.2)), 0.3, 3.0)
    return dict(residual_in=residual_in, gain_first=gain_first, gain_mixer=gain_mixer, gain_second=gain_second, gate_weight=gate_weight, gate_scale=gate_scale, up_weight=up_weight, up_scale=up_scale, down_weight=down_weight, down_scale=down_scale, query_weight=query_weight, query_scale=query_scale, key_weight=key_weight, key_scale=key_scale, value_weight=value_weight, value_scale=value_scale, output_weight=output_weight, output_scale=output_scale)


EPSILON = 1e-06
HEAD_FLOOR = 0.25
ROTARY_BASE = 10000.0
HIGHEST = lax.Precision.HIGHEST

def normalize(sequence_rows, gain_vector):
    values = sequence_rows.astype(jnp.float32)
    scaled = values * lax.rsqrt(lax.optimization_barrier(jnp.mean(values * values, axis=-1, keepdims=True)) + EPSILON)
    return (scaled * gain_vector).astype(jnp.bfloat16)

def head_rates(first_head, head_count, length):
    head_number = (first_head + jnp.arange(head_count)).astype(jnp.float32)
    return jnp.exp(jnp.log(1.0 / 16.0) + head_number / (HEADS - 1) * jnp.log(4.0 / length))

def rotate(values, positions):
    half_width = values.shape[-1] // 2
    frequency = ROTARY_BASE ** (-jnp.arange(half_width, dtype=jnp.float32) * 2.0 / values.shape[-1])
    angles = positions[:, None] * frequency[None, :]
    cosine = jnp.cos(angles)[:, None, :]
    sine_value = jnp.sin(angles)[:, None, :]
    front_half = values[..., :half_width]
    back_half = values[..., half_width:]
    return jnp.concatenate([front_half * cosine - back_half * sine_value, back_half * cosine + front_half * sine_value], axis=-1)

def retention(query_pre, key_pre, value_pre, decay_rates):
    length, head_count, head_width = query_pre.shape
    positions = jnp.arange(length, dtype=jnp.float32)
    query_rot = rotate(query_pre, positions).astype(jnp.bfloat16)
    key_rot = rotate(key_pre, positions).astype(jnp.bfloat16)
    value_low = value_pre.astype(jnp.bfloat16)
    blocks = length // BLOCK
    inside = jnp.arange(BLOCK, dtype=jnp.float32)
    distance = inside[:, None] - inside[None, :]
    within = jnp.where(distance >= 0, jnp.exp(-decay_rates[:, None, None] * jnp.maximum(distance, 0.0)), 0.0) * head_width ** (-0.5)
    query_blocks = query_rot.reshape(blocks, BLOCK, head_count, head_width)
    key_blocks = key_rot.reshape(blocks, BLOCK, head_count, head_width)
    value_blocks = value_low.reshape(blocks, BLOCK, head_count, head_width)
    scores = jnp.einsum('nihe,njhe->nhij', query_blocks.astype(jnp.float32), key_blocks.astype(jnp.float32), precision=HIGHEST)
    weights = (scores * within[None]).astype(jnp.bfloat16)
    inner_part = jnp.einsum('nhij,njhe->nihe', weights.astype(jnp.float32), value_blocks.astype(jnp.float32), precision=HIGHEST)
    fading = jnp.exp(-decay_rates[None, :] * (BLOCK - 1.0 - inside[:, None])) * head_width ** (-0.5)
    key_faded = key_blocks.astype(jnp.float32) * fading[None, :, :, None]
    updates = jnp.einsum('njhd,njhe->nhde', key_faded, value_blocks.astype(jnp.float32), precision=HIGHEST)
    block_decay = jnp.exp(-decay_rates * BLOCK)

    def advance(memory_state, update):
        return (memory_state * block_decay[:, None, None] + update, memory_state)
    _, before = lax.scan(advance, jnp.zeros((head_count, head_width, head_width), jnp.float32), updates)
    rising = jnp.exp(-decay_rates[None, :] * (inside[:, None] + 1.0))
    queried = query_blocks.astype(jnp.float32) * rising[None, :, :, None]
    carried_part = jnp.einsum('nihd,nhde->nihe', queried, before, precision=HIGHEST)
    combined = (inner_part + carried_part).reshape(length, head_count, head_width)
    normed = combined * lax.rsqrt(jnp.maximum(lax.optimization_barrier(jnp.mean(combined * combined, axis=-1, keepdims=True)), HEAD_FLOOR))
    return normed.astype(jnp.bfloat16).reshape(length, head_count * head_width)

def partial_sums(inputs, weight, factor, range_width):
    combined = jnp.zeros((inputs.shape[0], weight.shape[1]), jnp.float32)
    for member in range(N_TP):
        partial_piece = jnp.dot(inputs[:, member * range_width:(member + 1) * range_width], weight[member * range_width:(member + 1) * range_width], preferred_element_type=jnp.float32) * factor
        combined = combined + lax.optimization_barrier(partial_piece.astype(jnp.bfloat16)).astype(jnp.float32)
    return combined

def reference(residual_in, gain_first, gain_mixer, gain_second, gate_weight, gate_scale, up_weight, up_scale, down_weight, down_scale, query_weight, query_scale, key_weight, key_scale, value_weight, value_scale, output_weight, output_scale):
    gate_low = gate_weight.astype(jnp.bfloat16)
    up_low = up_weight.astype(jnp.bfloat16)
    down_low = down_weight.astype(jnp.bfloat16)
    query_low = query_weight.astype(jnp.bfloat16)
    key_low = key_weight.astype(jnp.bfloat16)
    value_low = value_weight.astype(jnp.bfloat16)
    output_low = output_weight.astype(jnp.bfloat16)
    decay_rates = head_rates(0, HEADS, TOK)

    def feed_forward(sequence_rows, gain_vector):
        normed = normalize(sequence_rows, gain_vector)
        gate_pre = jnp.dot(normed, gate_low, preferred_element_type=jnp.float32) * gate_scale
        up_pre = jnp.dot(normed, up_low, preferred_element_type=jnp.float32) * up_scale
        hidden = (jax.nn.silu(gate_pre) * up_pre).astype(jnp.bfloat16)
        return partial_sums(hidden, down_low, down_scale, FF // N_TP)

    def one_sequence(sequence_rows):
        middle = (sequence_rows.astype(jnp.float32) + 0.5 * feed_forward(sequence_rows, gain_first)).astype(jnp.bfloat16)
        mixer_input = normalize(middle, gain_mixer)
        query_pre = (jnp.dot(mixer_input, query_low, preferred_element_type=jnp.float32) * query_scale).reshape(TOK, HEADS, HEAD_DIM)
        key_pre = (jnp.dot(mixer_input, key_low, preferred_element_type=jnp.float32) * key_scale).reshape(TOK, HEADS, HEAD_DIM)
        value_pre = (jnp.dot(mixer_input, value_low, preferred_element_type=jnp.float32) * value_scale).reshape(TOK, HEADS, HEAD_DIM)
        mixed = retention(query_pre, key_pre, value_pre, decay_rates)
        mixer_out = partial_sums(mixed, output_low, output_scale, HEADS * HEAD_DIM // N_TP)
        second = (middle.astype(jnp.float32) + mixer_out).astype(jnp.bfloat16)
        return (second.astype(jnp.float32) + 0.5 * feed_forward(second, gain_second)).astype(jnp.bfloat16)
    sequences = residual_in.reshape(N_FS, TOK, D)
    return lax.map(one_sequence, sequences).reshape(N_FS * TOK, D)
```

```python
import jax
import jax.numpy as jnp
from jax import lax
from jax.sharding import Mesh
from jax.sharding import PartitionSpec as P

HEADS = 8
HEAD_DIM = 256
BLOCK = 64
FS = ("z", "y")
FS_TP = ("z", "y", "tp")


EPSILON = 1e-06
HEAD_FLOOR = 0.25
ROTARY_BASE = 10000.0
HIGHEST = lax.Precision.HIGHEST


def sent_to_all(x, axis):
    peers = lax.axis_size(axis)
    return lax.all_to_all(jnp.broadcast_to(x[None], (peers, *x.shape)), axis, 0, 0, tiled=True)


def in_order(pieces, dim):
    dims = list(pieces.shape[1:])
    dims[dim] *= pieces.shape[0]
    return jnp.moveaxis(pieces, 0, dim).reshape(dims)


def collect(x, axis, dim):
    pieces = sent_to_all(x, axis)
    return in_order(pieces, dim)


def split_up(x, dim, peers):
    dims = x.shape
    pieces = x.reshape(*dims[:dim], peers, dims[dim] // peers, *dims[dim + 1 :])
    return jnp.moveaxis(pieces, dim, 0)


def sent_and_summed(x, axis, dim):
    pieces = split_up(x, dim, lax.axis_size(axis))
    arrived = lax.all_to_all(pieces, axis, split_axis=0, concat_axis=0, tiled=True)
    return arrived.astype(jnp.float32).sum(axis=0)


def shifted(x, axis, by):
    peers = lax.axis_size(axis)
    return lax.ppermute(x, axis, [(i, (i + by) % peers) for i in range(peers)])


def after(x, first):
    return lax.optimization_barrier((x, first))[0]


def rows_over_y(part):
    half = part.shape[0] // 2
    below, above = shifted(part, "y", 1), shifted(part, "y", -1)
    far = jnp.concatenate([shifted(below[:half], "y", 1), shifted(above[half:], "y", -1)], axis=0)
    me = lax.axis_index("y")
    z, width = lax.axis_size("z"), part.shape[1]
    whole = jnp.zeros((z, 4, part.shape[0] // z, width), part.dtype)
    for piece, by in ((part, 0), (below, 3), (far, 2), (above, 1)):
        whole = lax.dynamic_update_slice(
            whole, piece.reshape(z, 1, -1, width), (0, (me + by) % 4, 0, 0)
        )
    return whole.reshape(-1, width)


def scaled_columns(weight, factor):
    low = weight.T.astype(jnp.bfloat16).astype(jnp.float32)
    return (low * factor[:, None]).astype(jnp.bfloat16)


def normalize(sequence_rows, gain_vector):
    values = sequence_rows.astype(jnp.float32)
    scaled = values * lax.rsqrt(jnp.mean(values * values, axis=-1, keepdims=True) + EPSILON)
    return (scaled * gain_vector).astype(jnp.bfloat16)


def collect_rows(sequence_rows, gain_vector):
    return collect(normalize(sequence_rows, gain_vector), "tp", 0)


def return_rows(inputs, weight):
    term = lax.dot_general(
        inputs, weight, (((1,), (1,)), ((), ())), preferred_element_type=jnp.float32
    )
    return sent_and_summed(
        lax.optimization_barrier(term.astype(jnp.bfloat16))
        .astype(jnp.float32)
        .astype(jnp.bfloat16),
        "tp",
        0,
    )


def head_rates(first_head, head_count, length):
    head_number = (first_head + jnp.arange(head_count)).astype(jnp.float32)
    return jnp.exp(jnp.log(1.0 / 16.0) + head_number / (HEADS - 1) * jnp.log(4.0 / length))


def rotate(values, positions):
    half_width = values.shape[-1] // 2
    frequency = ROTARY_BASE ** (-jnp.arange(half_width, dtype=jnp.float32) * 2.0 / values.shape[-1])
    angles = positions[:, None] * frequency[None, :]
    cosine = jnp.cos(angles)[:, None, :]
    sine_value = jnp.sin(angles)[:, None, :]
    front_half = values[..., :half_width]
    back_half = values[..., half_width:]
    return jnp.concatenate(
        [
            front_half * cosine - back_half * sine_value,
            back_half * cosine + front_half * sine_value,
        ],
        axis=-1,
    )


def retention(query_pre, key_pre, value_pre, decay_rates):
    length, head_count, head_width = query_pre.shape
    positions = jnp.arange(length, dtype=jnp.float32)
    query_rot = rotate(query_pre, positions).astype(jnp.bfloat16)
    key_rot = rotate(key_pre, positions).astype(jnp.bfloat16)
    value_low = value_pre.astype(jnp.bfloat16)
    blocks = length // BLOCK
    inside = jnp.arange(BLOCK, dtype=jnp.float32)
    distance = inside[:, None] - inside[None, :]
    within = jnp.where(
        distance >= 0, jnp.exp(-decay_rates[:, None, None] * jnp.maximum(distance, 0.0)), 0.0
    ) * head_width ** (-0.5)
    query_blocks = query_rot.reshape(blocks, BLOCK, head_count, head_width)
    key_blocks = key_rot.reshape(blocks, BLOCK, head_count, head_width)
    value_blocks = value_low.reshape(blocks, BLOCK, head_count, head_width)
    scores = jnp.einsum(
        "nihe,njhe->nhij", query_blocks, key_blocks, preferred_element_type=jnp.float32
    )
    weights = (scores * within[None]).astype(jnp.bfloat16)
    inner_part = jnp.einsum(
        "nhij,njhe->nihe", weights, value_blocks, preferred_element_type=jnp.float32
    )
    fading = jnp.exp(-decay_rates[None, :] * (BLOCK - 1.0 - inside[:, None])) * head_width ** (-0.5)
    key_faded = key_blocks.astype(jnp.float32) * fading[None, :, :, None]
    updates = jnp.einsum(
        "njhd,njhe->nhde", key_faded, value_blocks.astype(jnp.float32), precision=HIGHEST
    )
    block_decay = jnp.exp(-decay_rates * BLOCK)

    def advance(memory_state, update):
        return (memory_state * block_decay[:, None, None] + update, memory_state)

    _, before = lax.scan(
        advance, jnp.zeros((head_count, head_width, head_width), jnp.float32), updates
    )
    rising = jnp.exp(-decay_rates[None, :] * (inside[:, None] + 1.0))
    queried = query_blocks.astype(jnp.float32) * rising[None, :, :, None]
    carried_part = jnp.einsum("nihd,nhde->nihe", queried, before, precision=HIGHEST)
    combined = (inner_part + carried_part).reshape(length, head_count, head_width)
    normed = combined * lax.rsqrt(
        jnp.maximum(jnp.mean(combined * combined, axis=-1, keepdims=True), HEAD_FLOOR)
    )
    return normed.astype(jnp.bfloat16).reshape(length, head_count * head_width)


def body(
    residual_in,
    gain_first,
    gain_mixer,
    gain_second,
    gate_weight,
    gate_scale,
    up_weight,
    up_scale,
    down_weight,
    down_scale,
    query_weight,
    query_scale,
    key_weight,
    key_scale,
    value_weight,
    value_scale,
    output_weight,
    output_scale,
):
    low = jnp.bfloat16
    first_part = jnp.concatenate([gate_weight.astype(low), up_weight.astype(low)], axis=1)
    output_turned = scaled_columns(output_weight, output_scale)
    second_part = jnp.concatenate(
        [scaled_columns(down_weight, down_scale), output_turned[:, :128]], axis=1
    )
    third_part = jnp.concatenate(
        [
            query_weight.astype(low),
            key_weight.astype(low),
            value_weight.astype(low),
            output_turned[:, 128:],
        ],
        axis=1,
    )
    first_y = lax.all_gather(first_part, "y", axis=0, tiled=True)
    first_full = lax.all_gather(first_y, "z", axis=0, tiled=True)
    first_input = collect_rows(after(residual_in, first_y), gain_first)
    second_z = lax.all_gather(after(second_part, first_input), "z", axis=0, tiled=True)
    second_full = rows_over_y(second_z)
    third_z = lax.all_gather(after(third_part, second_z), "z", axis=0, tiled=True)
    third_full = rows_over_y(third_z)
    gate_full, up_full = first_full[:, : gate_weight.shape[1]], first_full[:, gate_weight.shape[1] :]
    hidden_width = down_weight.shape[0]
    down_full = second_full[:, :hidden_width]
    gate_pre = jnp.dot(first_input, gate_full, preferred_element_type=jnp.float32)
    up_pre = jnp.dot(first_input, up_full, preferred_element_type=jnp.float32)
    hidden_first = (jax.nn.silu(gate_pre * gate_scale) * (up_pre * up_scale)).astype(jnp.bfloat16)
    mlp_first = return_rows(hidden_first, down_full)
    middle = (residual_in.astype(jnp.float32) + 0.5 * mlp_first).astype(jnp.bfloat16)
    mixer_input = collect_rows(middle, gain_mixer)
    local_width = query_weight.shape[1]
    pieces = [third_full[:, k * local_width : (k + 1) * local_width] for k in range(3)]
    query_pre, key_pre, value_pre = tuple(
        (
            jnp.dot(mixer_input, pieces[member], preferred_element_type=jnp.float32)
            for member in range(3)
        )
    )
    output_full = jnp.concatenate(
        [second_full[:, hidden_width :], third_full[:, 3 * local_width :]], axis=1
    )
    length = mixer_input.shape[0]
    heads_local = local_width // HEAD_DIM
    decay_rates = head_rates(lax.axis_index("tp") * heads_local, heads_local, length)
    mixed = retention(
        (query_pre * query_scale).reshape(length, heads_local, HEAD_DIM),
        (key_pre * key_scale).reshape(length, heads_local, HEAD_DIM),
        (value_pre * value_scale).reshape(length, heads_local, HEAD_DIM),
        decay_rates,
    )
    mixer_out = return_rows(mixed, output_full)
    second = (middle.astype(jnp.float32) + mixer_out).astype(jnp.bfloat16)
    last_input = collect_rows(second, gain_second)
    gate_last = jnp.dot(last_input, gate_full, preferred_element_type=jnp.float32) * gate_scale
    up_last = jnp.dot(last_input, up_full, preferred_element_type=jnp.float32) * up_scale
    hidden_second = (jax.nn.silu(gate_last) * up_last).astype(jnp.bfloat16)
    mlp_second = return_rows(hidden_second, down_full)
    return (second.astype(jnp.float32) + 0.5 * mlp_second).astype(jnp.bfloat16)


def solution(mesh):
    split = Mesh(mesh.devices.reshape(16, 4, mesh.shape["tp"]), ("z", "y", "tp"))
    in_specs = (
        P(FS_TP, None),
        P(),
        P(),
        P(),
        P(FS, "tp"),
        P("tp"),
        P(FS, "tp"),
        P("tp"),
        P("tp", FS),
        P(FS),
        P(FS, "tp"),
        P("tp"),
        P(FS, "tp"),
        P("tp"),
        P(FS, "tp"),
        P("tp"),
        P("tp", FS),
        P(FS),
    )
    out_specs = P(FS_TP, None)
    return jax.shard_map(body, mesh=split, in_specs=in_specs, out_specs=out_specs, check_vma=False)
```

```python
import jax
import jax.numpy as jnp
from jax import lax
from jax.sharding import Mesh
from jax.sharding import PartitionSpec as P

HEADS = 8
HEAD_DIM = 256
BLOCK = 64
FS = ("z", "y")
FS_TP = ("z", "y", "tp")


EPSILON = 1e-06
HEAD_FLOOR = 0.25
ROTARY_BASE = 10000.0
HIGHEST = lax.Precision.HIGHEST


def sent_to_all(x, axis):
    peers = lax.axis_size(axis)
    return lax.all_to_all(jnp.broadcast_to(x[None], (peers, *x.shape)), axis, 0, 0, tiled=True)


def shifted(x, axis, by):
    peers = lax.axis_size(axis)
    return lax.ppermute(x, axis, [(i, (i + by) % peers) for i in range(peers)])


def after(x, first):
    return lax.optimization_barrier((x, first))[0]


def y_neighbours(part):
    return shifted(part, "y", 1), shifted(part, "y", -1)


def y_opposite(below, above):
    half = below.shape[0] // 2
    return shifted(below[:half], "y", 1), shifted(above[half:], "y", -1)


def joined_over_y(part, below, above, far):
    me = lax.axis_index("y")
    z, width = lax.axis_size("z"), part.shape[1]
    own = part.reshape(z, 1, -1, width)
    whole = jnp.broadcast_to(own, (z, 4, own.shape[2], width))
    far = jnp.concatenate(far, axis=0)
    for piece, by in ((below, 3), (far, 2), (above, 1)):
        whole = lax.dynamic_update_slice(
            whole, piece.reshape(own.shape), (0, (me + by) % 4, 0, 0)
        )
    return whole.reshape(-1, width)


def scaled_columns(weight, factor):
    low = weight.T.astype(jnp.bfloat16).astype(jnp.float32)
    return (low * factor[:, None]).astype(jnp.bfloat16)


def normalize(sequence_rows, gain_vector):
    values = sequence_rows.astype(jnp.float32)
    scaled = values * lax.rsqrt(jnp.mean(values * values, axis=-1, keepdims=True) + EPSILON)
    return (scaled * gain_vector).astype(jnp.bfloat16)


def collect_rows(own_rows, gain_vector):
    return sent_to_all(normalize(own_rows, gain_vector), "tp").reshape(-1, own_rows.shape[1])


def partial_rows(inputs, weight):
    term = lax.dot_general(
        inputs, weight, (((1,), (1,)), ((), ())), preferred_element_type=jnp.float32
    )
    return lax.optimization_barrier(term.astype(jnp.bfloat16))


def summed_rows(term):
    pieces = term.reshape(lax.axis_size("tp"), -1, term.shape[1])
    arrived = lax.all_to_all(pieces, "tp", split_axis=0, concat_axis=0, tiled=True)
    return arrived.astype(jnp.float32).sum(axis=0)


def head_rates(first_head, head_count, length):
    head_number = (first_head + jnp.arange(head_count)).astype(jnp.float32)
    return jnp.exp(jnp.log(1.0 / 16.0) + head_number / (HEADS - 1) * jnp.log(4.0 / length))


def rotate(values, positions):
    half_width = values.shape[-1] // 2
    frequency = ROTARY_BASE ** (-jnp.arange(half_width, dtype=jnp.float32) * 2.0 / values.shape[-1])
    angles = positions[:, None] * frequency[None, :]
    cosine = jnp.cos(angles)[:, None, :]
    sine_value = jnp.sin(angles)[:, None, :]
    front_half = values[..., :half_width]
    back_half = values[..., half_width:]
    return jnp.concatenate(
        [
            front_half * cosine - back_half * sine_value,
            back_half * cosine + front_half * sine_value,
        ],
        axis=-1,
    )


def retention(query_pre, key_pre, value_pre, decay_rates):
    length, head_count, head_width = query_pre.shape
    positions = jnp.arange(length, dtype=jnp.float32)
    query_rot = rotate(query_pre, positions).astype(jnp.bfloat16)
    key_rot = rotate(key_pre, positions).astype(jnp.bfloat16)
    value_low = value_pre.astype(jnp.bfloat16)
    blocks = length // BLOCK
    inside = jnp.arange(BLOCK, dtype=jnp.float32)
    distance = inside[:, None] - inside[None, :]
    within = jnp.where(
        distance >= 0, jnp.exp(-decay_rates[:, None, None] * jnp.maximum(distance, 0.0)), 0.0
    ) * head_width ** (-0.5)
    query_blocks = query_rot.reshape(blocks, BLOCK, head_count, head_width)
    key_blocks = key_rot.reshape(blocks, BLOCK, head_count, head_width)
    value_blocks = value_low.reshape(blocks, BLOCK, head_count, head_width)
    scores = jnp.einsum(
        "nihe,njhe->nhij", query_blocks, key_blocks, preferred_element_type=jnp.float32
    )
    weights = (scores * within[None]).astype(jnp.bfloat16)
    inner_part = jnp.einsum(
        "nhij,njhe->nihe", weights, value_blocks, preferred_element_type=jnp.float32
    )
    fading = jnp.exp(-decay_rates[None, :] * (BLOCK - 1.0 - inside[:, None])) * head_width ** (-0.5)
    key_faded = key_blocks.astype(jnp.float32) * fading[None, :, :, None]
    updates = jnp.einsum(
        "njhd,njhe->nhde", key_faded, value_blocks.astype(jnp.float32), precision=HIGHEST
    )
    block_decay = jnp.exp(-decay_rates * BLOCK)

    def advance(memory_state, update):
        return (memory_state * block_decay[:, None, None] + update, memory_state)

    _, before = lax.scan(
        advance, jnp.zeros((head_count, head_width, head_width), jnp.float32), updates
    )
    rising = jnp.exp(-decay_rates[None, :] * (inside[:, None] + 1.0))
    queried = query_blocks.astype(jnp.float32) * rising[None, :, :, None]
    carried_part = jnp.einsum("nihd,nhde->nihe", queried, before, precision=HIGHEST)
    combined = (inner_part + carried_part).reshape(length, head_count, head_width)
    normed = combined * lax.rsqrt(
        jnp.maximum(jnp.mean(combined * combined, axis=-1, keepdims=True), HEAD_FLOOR)
    )
    return normed.astype(jnp.bfloat16).reshape(length, head_count * head_width)


def body(
    residual_in,
    gain_first,
    gain_mixer,
    gain_second,
    gate_weight,
    gate_scale,
    up_weight,
    up_scale,
    down_weight,
    down_scale,
    query_weight,
    query_scale,
    key_weight,
    key_scale,
    value_weight,
    value_scale,
    output_weight,
    output_scale,
):
    low = jnp.bfloat16
    first_part = jnp.concatenate([gate_weight.astype(low), up_weight.astype(low)], axis=1)
    output_turned = scaled_columns(output_weight, output_scale)
    second_part = jnp.concatenate(
        [scaled_columns(down_weight, down_scale), output_turned[:, :128]], axis=1
    )
    third_part = jnp.concatenate(
        [
            query_weight.astype(low),
            key_weight.astype(low),
            value_weight.astype(low),
            output_turned[:, 128:],
        ],
        axis=1,
    )
    first_y = lax.all_gather(first_part, "y", axis=0, tiled=True)
    first_full = lax.all_gather(first_y, "z", axis=0, tiled=True)
    first_input = collect_rows(after(residual_in, first_y), gain_first)
    second_z = lax.all_gather(after(second_part, first_y), "z", axis=0, tiled=True)
    second_near = y_neighbours(second_z)
    third_z = lax.all_gather(after(third_part, second_z), "z", axis=0, tiled=True)
    second_far = y_opposite(*second_near)
    third_near = y_neighbours(after(third_z, second_near))
    third_far = y_opposite(*third_near)
    second_full = joined_over_y(second_z, *second_near, second_far)
    hidden_width = down_weight.shape[0]
    gate_full, up_full = first_full[:, :hidden_width], first_full[:, hidden_width:]
    down_full = second_full[:, :hidden_width]
    def feed_forward(inputs):
        gate = jnp.dot(inputs, gate_full, preferred_element_type=jnp.float32) * gate_scale
        up = jnp.dot(inputs, up_full, preferred_element_type=jnp.float32) * up_scale
        return partial_rows((jax.nn.silu(gate) * up).astype(low), down_full)

    first_term = feed_forward(first_input)
    third_full = joined_over_y(*after((third_z, *third_near, third_far), first_term))
    local_width = query_weight.shape[1]
    query_full, key_full, value_full = [
        third_full[:, k * local_width : (k + 1) * local_width] for k in range(3)
    ]
    output_full = jnp.concatenate(
        [second_full[:, hidden_width:], third_full[:, 3 * local_width :]], axis=1
    )

    def projected(inputs):
        query = jnp.dot(inputs, query_full, preferred_element_type=jnp.float32) * query_scale
        key = jnp.dot(inputs, key_full, preferred_element_type=jnp.float32) * key_scale
        value = jnp.dot(inputs, value_full, preferred_element_type=jnp.float32) * value_scale
        return query, key, value

    mlp_first = summed_rows(first_term)
    middle = (residual_in.astype(jnp.float32) + 0.5 * mlp_first).astype(low)
    heads_local = local_width // HEAD_DIM
    query_pre, key_pre, value_pre = [
        a.reshape(-1, heads_local, HEAD_DIM) for a in projected(collect_rows(middle, gain_mixer))
    ]
    decay_rates = head_rates(
        lax.axis_index("tp") * heads_local, heads_local, query_pre.shape[0]
    )
    mixed = retention(query_pre, key_pre, value_pre, decay_rates)
    second = (middle.astype(jnp.float32) + summed_rows(partial_rows(mixed, output_full))).astype(low)
    mlp_second = summed_rows(feed_forward(collect_rows(second, gain_second)))
    return (second.astype(jnp.float32) + 0.5 * mlp_second).astype(low)


def solution(mesh):
    split = Mesh(mesh.devices.reshape(16, 4, mesh.shape["tp"]), ("z", "y", "tp"))
    in_specs = (
        P(FS_TP, None),
        P(),
        P(),
        P(),
        P(FS, "tp"),
        P("tp"),
        P(FS, "tp"),
        P("tp"),
        P("tp", FS),
        P(FS),
        P(FS, "tp"),
        P("tp"),
        P(FS, "tp"),
        P("tp"),
        P(FS, "tp"),
        P("tp"),
        P("tp", FS),
        P(FS),
    )
    out_specs = P(FS_TP, None)
    return jax.shard_map(body, mesh=split, in_specs=in_specs, out_specs=out_specs, check_vma=False)
```

```python
import jax
import jax.numpy as jnp
from jax import lax
from jax.sharding import Mesh
from jax.sharding import PartitionSpec as P

HEADS = 8
HEAD_DIM = 256
BLOCK = 64
FS = ("z", "y")
FS_TP = ("z", "y", "tp")


EPSILON = 1e-06
HEAD_FLOOR = 0.25
ROTARY_BASE = 10000.0
HIGHEST = lax.Precision.HIGHEST


def sent_to_all(x, axis):
    peers = lax.axis_size(axis)
    return lax.all_to_all(jnp.broadcast_to(x[None], (peers, *x.shape)), axis, 0, 0, tiled=True)


def shifted(x, axis, by):
    peers = lax.axis_size(axis)
    return lax.ppermute(x, axis, [(i, (i + by) % peers) for i in range(peers)])


def after(x, first):
    return lax.optimization_barrier((x, first))[0]


def y_neighbours(part):
    return shifted(part, "y", 1), shifted(part, "y", -1)


def y_opposite(below, above):
    half = below.shape[0] // 2
    return shifted(below[:half], "y", 1), shifted(above[half:], "y", -1)


def joined_over_y(part, below, above, far):
    me = lax.axis_index("y")
    own = part[:, :, None]
    whole = jnp.broadcast_to(own, (*part.shape[:2], lax.axis_size("y"), *part.shape[2:]))
    for piece, by in ((below, 3), (far, 2), (above, 1)):
        place = (0, 0, (me + by) % lax.axis_size("y"), 0, 0)
        whole = lax.dynamic_update_slice(whole, piece[:, :, None], place)
    return whole


def scaled_columns(weight, factor):
    low = weight.T.astype(jnp.bfloat16).astype(jnp.float32)
    return (low * factor[:, None]).astype(jnp.bfloat16)


def normalize(sequence_rows, gain_vector):
    values = sequence_rows.astype(jnp.float32)
    scaled = values * lax.rsqrt(jnp.mean(values * values, axis=-1, keepdims=True) + EPSILON)
    return (scaled * gain_vector).astype(jnp.bfloat16)


def collect_rows(own_rows, gain_vector):
    return sent_to_all(normalize(own_rows, gain_vector), "tp").reshape(-1, own_rows.shape[1])


def partial_rows(inputs, weight):
    term = lax.dot_general(
        inputs, weight, (((1,), (1,)), ((), ())), preferred_element_type=jnp.float32
    )
    return lax.optimization_barrier(term.astype(jnp.bfloat16))


def summed_rows(term):
    pieces = term.reshape(lax.axis_size("tp"), -1, term.shape[1])
    arrived = lax.all_to_all(pieces, "tp", split_axis=0, concat_axis=0, tiled=True)
    return arrived.astype(jnp.float32).sum(axis=0)


def head_rates(first_head, head_count, length):
    head_number = (first_head + jnp.arange(head_count)).astype(jnp.float32)
    return jnp.exp(jnp.log(1.0 / 16.0) + head_number / (HEADS - 1) * jnp.log(4.0 / length))


def rotate(values, positions):
    half_width = values.shape[-1] // 2
    frequency = ROTARY_BASE ** (-jnp.arange(half_width, dtype=jnp.float32) * 2.0 / values.shape[-1])
    angles = positions[:, None] * frequency[None, :]
    cosine = jnp.cos(angles)[:, None, :]
    sine_value = jnp.sin(angles)[:, None, :]
    front_half = values[..., :half_width]
    back_half = values[..., half_width:]
    return jnp.concatenate(
        [
            front_half * cosine - back_half * sine_value,
            back_half * cosine + front_half * sine_value,
        ],
        axis=-1,
    )


def retention(query_pre, key_pre, value_pre, decay_rates):
    length, head_count, head_width = query_pre.shape
    positions = jnp.arange(length, dtype=jnp.float32)
    query_rot = rotate(query_pre, positions).astype(jnp.bfloat16)
    key_rot = rotate(key_pre, positions).astype(jnp.bfloat16)
    value_low = value_pre.astype(jnp.bfloat16)
    blocks = length // BLOCK
    inside = jnp.arange(BLOCK, dtype=jnp.float32)
    distance = inside[:, None] - inside[None, :]
    within = jnp.where(
        distance >= 0, jnp.exp(-decay_rates[:, None, None] * jnp.maximum(distance, 0.0)), 0.0
    ) * head_width ** (-0.5)
    query_blocks = query_rot.reshape(blocks, BLOCK, head_count, head_width)
    key_blocks = key_rot.reshape(blocks, BLOCK, head_count, head_width)
    value_blocks = value_low.reshape(blocks, BLOCK, head_count, head_width)
    scores = jnp.einsum(
        "nihe,njhe->nhij", query_blocks, key_blocks, preferred_element_type=jnp.float32
    )
    weights = (scores * within[None]).astype(jnp.bfloat16)
    inner_part = jnp.einsum(
        "nhij,njhe->nihe", weights, value_blocks, preferred_element_type=jnp.float32
    )
    fading = jnp.exp(-decay_rates[None, :] * (BLOCK - 1.0 - inside[:, None])) * head_width ** (-0.5)
    key_faded = key_blocks.astype(jnp.float32) * fading[None, :, :, None]
    updates = jnp.einsum(
        "njhd,njhe->nhde", key_faded, value_blocks.astype(jnp.float32), precision=HIGHEST
    )
    block_decay = jnp.exp(-decay_rates * BLOCK)

    def advance(memory_state, update):
        return (memory_state * block_decay[:, None, None] + update, memory_state)

    _, before = lax.scan(
        advance, jnp.zeros((head_count, head_width, head_width), jnp.float32), updates
    )
    rising = jnp.exp(-decay_rates[None, :] * (inside[:, None] + 1.0))
    queried = query_blocks.astype(jnp.float32) * rising[None, :, :, None]
    carried_part = jnp.einsum("nihd,nhde->nihe", queried, before, precision=HIGHEST)
    combined = (inner_part + carried_part).reshape(length, head_count, head_width)
    normed = combined * lax.rsqrt(
        jnp.maximum(jnp.mean(combined * combined, axis=-1, keepdims=True), HEAD_FLOOR)
    )
    return normed.astype(jnp.bfloat16).reshape(length, head_count * head_width)


def body(
    residual_in,
    gain_first,
    gain_mixer,
    gain_second,
    gate_weight,
    gate_scale,
    up_weight,
    up_scale,
    down_weight,
    down_scale,
    query_weight,
    query_scale,
    key_weight,
    key_scale,
    value_weight,
    value_scale,
    output_weight,
    output_scale,
):
    low = jnp.bfloat16
    z, rows = lax.axis_size("z"), gate_weight.shape[0]
    hidden_width, local_width = down_weight.shape[0], query_weight.shape[1]
    first_part = jnp.concatenate([gate_weight.astype(low), up_weight.astype(low)], axis=1)
    second_part = scaled_columns(down_weight, down_scale)
    third_part = jnp.concatenate(
        [
            query_weight.astype(low),
            key_weight.astype(low),
            value_weight.astype(low),
            scaled_columns(output_weight, output_scale),
        ],
        axis=0,
    )
    first_y = lax.all_gather(first_part, "y", axis=0, tiled=True)
    whole_z = lax.all_gather(
        jnp.concatenate([first_y, third_part], axis=1), "z", axis=0, tiled=True
    )
    gate_full = whole_z[:, :hidden_width]
    up_full = whole_z[:, hidden_width : 2 * hidden_width]
    first_input = collect_rows(after(residual_in, first_y), gain_first)
    second_z = lax.all_gather(after(second_part, first_y), "z", axis=0, tiled=True)
    second_near = y_neighbours(second_z)
    second_far = y_opposite(*second_near)
    third_z = whole_z[:, 2 * hidden_width :]
    third_near = y_neighbours(third_z)
    third_far = y_opposite(*third_near)
    down_full = joined_over_y(
        *[
            x.reshape(1, z, rows, hidden_width)
            for x in (second_z, *second_near, jnp.concatenate(second_far, axis=0))
        ]
    ).reshape(-1, hidden_width)

    def feed_forward(inputs):
        gate = jnp.dot(inputs, gate_full, preferred_element_type=jnp.float32) * gate_scale
        up = jnp.dot(inputs, up_full, preferred_element_type=jnp.float32) * up_scale
        return partial_rows((jax.nn.silu(gate) * up).astype(low), down_full)

    first_term = feed_forward(first_input)
    third_pieces = after((third_z, *third_near, jnp.concatenate(third_far, axis=0)), first_term)
    third_full = joined_over_y(
        *[x.reshape(z, 4, rows, local_width).swapaxes(0, 1) for x in third_pieces]
    )
    query_full, key_full, value_full, output_full = [
        third_full[k].reshape(-1, local_width) for k in range(4)
    ]

    def projected(inputs):
        query = jnp.dot(inputs, query_full, preferred_element_type=jnp.float32) * query_scale
        key = jnp.dot(inputs, key_full, preferred_element_type=jnp.float32) * key_scale
        value = jnp.dot(inputs, value_full, preferred_element_type=jnp.float32) * value_scale
        return query, key, value

    mlp_first = summed_rows(first_term)
    middle = (residual_in.astype(jnp.float32) + 0.5 * mlp_first).astype(low)
    heads_local = local_width // HEAD_DIM
    query_pre, key_pre, value_pre = [
        a.reshape(-1, heads_local, HEAD_DIM) for a in projected(collect_rows(middle, gain_mixer))
    ]
    decay_rates = head_rates(
        lax.axis_index("tp") * heads_local, heads_local, query_pre.shape[0]
    )
    mixed = retention(query_pre, key_pre, value_pre, decay_rates)
    second = (middle.astype(jnp.float32) + summed_rows(partial_rows(mixed, output_full))).astype(low)
    mlp_second = summed_rows(feed_forward(collect_rows(second, gain_second)))
    return (second.astype(jnp.float32) + 0.5 * mlp_second).astype(low)


def solution(mesh):
    split = Mesh(mesh.devices.reshape(16, 4, mesh.shape["tp"]), ("z", "y", "tp"))
    in_specs = (
        P(FS_TP, None),
        P(),
        P(),
        P(),
        P(FS, "tp"),
        P("tp"),
        P(FS, "tp"),
        P("tp"),
        P("tp", FS),
        P(FS),
        P(FS, "tp"),
        P("tp"),
        P(FS, "tp"),
        P("tp"),
        P(FS, "tp"),
        P("tp"),
        P("tp", FS),
        P(FS),
    )
    out_specs = P(FS_TP, None)
    return jax.shard_map(body, mesh=split, in_specs=in_specs, out_specs=out_specs, check_vma=False)
```

```python
import jax
import jax.numpy as jnp
from jax import lax
from jax.sharding import Mesh
from jax.sharding import PartitionSpec as P

HEADS = 8
HEAD_DIM = 256
BLOCK = 64
FS = ("z", "y")
FS_TP = ("z", "y", "tp")


EPSILON = 1e-06
HEAD_FLOOR = 0.25
ROTARY_BASE = 10000.0
HIGHEST = lax.Precision.HIGHEST


def sent_to_all(x, axis):
    peers = lax.axis_size(axis)
    return lax.all_to_all(jnp.broadcast_to(x[None], (peers, *x.shape)), axis, 0, 0, tiled=True)


def shifted(x, axis, by):
    peers = lax.axis_size(axis)
    return lax.ppermute(x, axis, [(i, (i + by) % peers) for i in range(peers)])


def after(x, first):
    return lax.optimization_barrier((x, first))[0]


def y_neighbours(part):
    return shifted(part, "y", 1), shifted(part, "y", -1)


def y_opposite(below, above):
    half = below.shape[0] // 2
    return shifted(below[:half], "y", 1), shifted(above[half:], "y", -1)


def joined_over_y(part, below, above, far):
    me, peers = lax.axis_index("y"), lax.axis_size("y")
    whole = jnp.broadcast_to(part[:, None], (part.shape[0], peers, *part.shape[1:]))
    for piece, by in ((below, 3), (far, 2), (above, 1)):
        whole = lax.dynamic_update_slice(whole, piece[:, None], (0, (me + by) % peers, 0, 0))
    return whole.reshape(-1, part.shape[2])


def scaled_columns(weight, factor):
    low = weight.T.astype(jnp.bfloat16).astype(jnp.float32)
    return (low * factor[:, None]).astype(jnp.bfloat16)


def normalize(sequence_rows, gain_vector):
    values = sequence_rows.astype(jnp.float32)
    scaled = values * lax.rsqrt(jnp.mean(values * values, axis=-1, keepdims=True) + EPSILON)
    return (scaled * gain_vector).astype(jnp.bfloat16)


def collect_rows(own_rows, gain_vector):
    return sent_to_all(normalize(own_rows, gain_vector), "tp").reshape(-1, own_rows.shape[1])


def partial_rows(inputs, weight):
    term = lax.dot_general(
        inputs, weight, (((1,), (1,)), ((), ())), preferred_element_type=jnp.float32
    )
    return lax.optimization_barrier(term.astype(jnp.bfloat16))


def summed_rows(term):
    pieces = term.reshape(lax.axis_size("tp"), -1, term.shape[1])
    arrived = lax.all_to_all(pieces, "tp", split_axis=0, concat_axis=0, tiled=True)
    return arrived.astype(jnp.float32).sum(axis=0)


def head_rates(first_head, head_count, length):
    head_number = (first_head + jnp.arange(head_count)).astype(jnp.float32)
    return jnp.exp(jnp.log(1.0 / 16.0) + head_number / (HEADS - 1) * jnp.log(4.0 / length))


def rotate(values, positions):
    half_width = values.shape[-1] // 2
    frequency = ROTARY_BASE ** (-jnp.arange(half_width, dtype=jnp.float32) * 2.0 / values.shape[-1])
    angles = positions[:, None] * frequency[None, :]
    cosine = jnp.cos(angles)[:, None, :]
    sine_value = jnp.sin(angles)[:, None, :]
    front_half = values[..., :half_width]
    back_half = values[..., half_width:]
    return jnp.concatenate(
        [
            front_half * cosine - back_half * sine_value,
            back_half * cosine + front_half * sine_value,
        ],
        axis=-1,
    )


def retention(query_pre, key_pre, value_pre, decay_rates):
    length, head_count, head_width = query_pre.shape
    positions = jnp.arange(length, dtype=jnp.float32)
    query_rot = rotate(query_pre, positions).astype(jnp.bfloat16)
    key_rot = rotate(key_pre, positions).astype(jnp.bfloat16)
    value_low = value_pre.astype(jnp.bfloat16)
    blocks = length // BLOCK
    inside = jnp.arange(BLOCK, dtype=jnp.float32)
    distance = inside[:, None] - inside[None, :]
    within = jnp.where(
        distance >= 0, jnp.exp(-decay_rates[:, None, None] * jnp.maximum(distance, 0.0)), 0.0
    ) * head_width ** (-0.5)
    query_blocks = query_rot.reshape(blocks, BLOCK, head_count, head_width)
    key_blocks = key_rot.reshape(blocks, BLOCK, head_count, head_width)
    value_blocks = value_low.reshape(blocks, BLOCK, head_count, head_width)
    scores = jnp.einsum(
        "nihe,njhe->nhij", query_blocks, key_blocks, preferred_element_type=jnp.float32
    )
    weights = (scores * within[None]).astype(jnp.bfloat16)
    inner_part = jnp.einsum(
        "nhij,njhe->nihe", weights, value_blocks, preferred_element_type=jnp.float32
    )
    fading = jnp.exp(-decay_rates[None, :] * (BLOCK - 1.0 - inside[:, None])) * head_width ** (-0.5)
    key_faded = key_blocks.astype(jnp.float32) * fading[None, :, :, None]
    updates = jnp.einsum(
        "njhd,njhe->nhde", key_faded, value_blocks.astype(jnp.float32), precision=HIGHEST
    )
    block_decay = jnp.exp(-decay_rates * BLOCK)

    def advance(memory_state, update):
        return (memory_state * block_decay[:, None, None] + update, memory_state)

    _, before = lax.scan(
        advance, jnp.zeros((head_count, head_width, head_width), jnp.float32), updates
    )
    rising = jnp.exp(-decay_rates[None, :] * (inside[:, None] + 1.0))
    queried = query_blocks.astype(jnp.float32) * rising[None, :, :, None]
    carried_part = jnp.einsum("nihd,nhde->nihe", queried, before, precision=HIGHEST)
    combined = (inner_part + carried_part).reshape(length, head_count, head_width)
    normed = combined * lax.rsqrt(
        jnp.maximum(jnp.mean(combined * combined, axis=-1, keepdims=True), HEAD_FLOOR)
    )
    return normed.astype(jnp.bfloat16).reshape(length, head_count * head_width)


def body(
    residual_in,
    gain_first,
    gain_mixer,
    gain_second,
    gate_weight,
    gate_scale,
    up_weight,
    up_scale,
    down_weight,
    down_scale,
    query_weight,
    query_scale,
    key_weight,
    key_scale,
    value_weight,
    value_scale,
    output_weight,
    output_scale,
):
    low = jnp.bfloat16
    z, rows = lax.axis_size("z"), gate_weight.shape[0]
    hidden_width, local_width = down_weight.shape[0], query_weight.shape[1]
    first_part = jnp.concatenate([gate_weight.astype(low), up_weight.astype(low)], axis=1)
    second_part = scaled_columns(down_weight, down_scale)
    third_part = jnp.concatenate(
        [
            query_weight.astype(low),
            key_weight.astype(low),
            value_weight.astype(low),
            scaled_columns(output_weight, output_scale),
        ],
        axis=1,
    )
    first_y = lax.all_gather(first_part, "y", axis=0, tiled=True)
    first_full = lax.all_gather(first_y, "z", axis=0, tiled=True)
    gate_full, up_full = first_full[:, :hidden_width], first_full[:, hidden_width:]
    second_z = lax.all_gather(after(second_part, first_y), "z", axis=0, tiled=True)
    second_near = y_neighbours(second_z)
    first_input = collect_rows(after(residual_in, second_z), gain_first)
    third_y = lax.all_gather(after(third_part, second_z), "y", axis=0, tiled=True)
    third_full = lax.all_gather(third_y, "z", axis=0, tiled=True)
    query_full, key_full, value_full, output_full = [
        third_full[:, k * local_width : (k + 1) * local_width] for k in range(4)
    ]
    second_far = y_opposite(*second_near)
    down_full = joined_over_y(
        *[
            x.reshape(z, rows, hidden_width)
            for x in (second_z, *second_near, jnp.concatenate(second_far, axis=0))
        ]
    )

    def feed_forward(inputs):
        gate = jnp.dot(inputs, gate_full, preferred_element_type=jnp.float32) * gate_scale
        up = jnp.dot(inputs, up_full, preferred_element_type=jnp.float32) * up_scale
        return partial_rows((jax.nn.silu(gate) * up).astype(low), down_full)

    first_term = feed_forward(first_input)
    def projected(inputs):
        query = jnp.dot(inputs, query_full, preferred_element_type=jnp.float32) * query_scale
        key = jnp.dot(inputs, key_full, preferred_element_type=jnp.float32) * key_scale
        value = jnp.dot(inputs, value_full, preferred_element_type=jnp.float32) * value_scale
        return query, key, value

    mlp_first = summed_rows(first_term)
    middle = (residual_in.astype(jnp.float32) + 0.5 * mlp_first).astype(low)
    heads_local = local_width // HEAD_DIM
    query_pre, key_pre, value_pre = [
        a.reshape(-1, heads_local, HEAD_DIM) for a in projected(collect_rows(middle, gain_mixer))
    ]
    decay_rates = head_rates(
        lax.axis_index("tp") * heads_local, heads_local, query_pre.shape[0]
    )
    mixed = retention(query_pre, key_pre, value_pre, decay_rates)
    second = (middle.astype(jnp.float32) + summed_rows(partial_rows(mixed, output_full))).astype(low)
    mlp_second = summed_rows(feed_forward(collect_rows(second, gain_second)))
    return (second.astype(jnp.float32) + 0.5 * mlp_second).astype(low)


def solution(mesh):
    split = Mesh(mesh.devices.reshape(16, 4, mesh.shape["tp"]), ("z", "y", "tp"))
    in_specs = (
        P(FS_TP, None),
        P(),
        P(),
        P(),
        P(FS, "tp"),
        P("tp"),
        P(FS, "tp"),
        P("tp"),
        P("tp", FS),
        P(FS),
        P(FS, "tp"),
        P("tp"),
        P(FS, "tp"),
        P("tp"),
        P(FS, "tp"),
        P("tp"),
        P("tp", FS),
        P(FS),
    )
    out_specs = P(FS_TP, None)
    return jax.shard_map(body, mesh=split, in_specs=in_specs, out_specs=out_specs, check_vma=False)
```

```python
import jax
import jax.numpy as jnp
from jax import lax
from jax.experimental import pallas as pl
from jax.experimental.pallas import tpu as pltpu
from jax.sharding import Mesh
from jax.sharding import PartitionSpec as P

HEADS = 8
HEAD_DIM = 256
BLOCK = 64
TOK = 256
FS = ("z", "y")
FS_TP = ("z", "y", "tp")


EPSILON = 1e-06
HEAD_FLOOR = 0.25
ROTARY_BASE = 10000.0
HIGHEST = lax.Precision.HIGHEST


def sent_to_all(x, axis):
    peers = lax.axis_size(axis)
    return lax.all_to_all(jnp.broadcast_to(x[None], (peers, *x.shape)), axis, 0, 0, tiled=True)


def shifted(x, axis, by):
    peers = lax.axis_size(axis)
    return lax.ppermute(x, axis, [(i, (i + by) % peers) for i in range(peers)])


def after(x, first):
    return lax.optimization_barrier((x, first))[0]


def y_neighbours(part):
    return shifted(part, "y", 1), shifted(part, "y", -1)


def y_opposite(below, above):
    half = below.shape[0] // 2
    return shifted(below[:half], "y", 1), shifted(above[half:], "y", -1)


def joined_over_y(part, below, above, far):
    me, peers = lax.axis_index("y"), lax.axis_size("y")
    whole = jnp.broadcast_to(part[:, None], (part.shape[0], peers, *part.shape[1:]))
    for piece, by in ((below, 3), (far, 2), (above, 1)):
        whole = lax.dynamic_update_slice(whole, piece[:, None], (0, (me + by) % peers, 0, 0))
    return whole.reshape(-1, part.shape[2])


def scaled_columns(weight, factor):
    low = weight.T.astype(jnp.bfloat16).astype(jnp.float32)
    return (low * factor[:, None]).astype(jnp.bfloat16)


def normalize(sequence_rows, gain_vector):
    values = sequence_rows.astype(jnp.float32)
    scaled = values * lax.rsqrt(jnp.mean(values * values, axis=-1, keepdims=True) + EPSILON)
    return (scaled * gain_vector).astype(jnp.bfloat16)


def collect_rows(own_rows, gain_vector):
    return sent_to_all(normalize(own_rows, gain_vector), "tp").reshape(-1, own_rows.shape[1])


def product(inputs, turned):
    return lax.dot_general(
        inputs, turned, (((1,), (1,)), ((), ())), preferred_element_type=jnp.float32
    )


def summed_rows(term):
    pieces = term.reshape(lax.axis_size("tp"), -1, term.shape[1])
    arrived = lax.all_to_all(pieces, "tp", split_axis=0, concat_axis=0, tiled=True)
    return arrived.astype(jnp.float32).sum(axis=0)


def head_rates(first_head, head_count, length):
    head_number = (first_head + jnp.arange(head_count)).astype(jnp.float32)
    return jnp.exp(jnp.log(1.0 / 16.0) + head_number / (HEADS - 1) * jnp.log(4.0 / length))


def mlp_kernel(x_ref, gate_ref, up_ref, down_ref, gate_scale_ref, up_scale_ref, out_ref, total):
    step = pl.program_id(0)
    x = x_ref[...]
    gate = jnp.dot(x, gate_ref[...], preferred_element_type=jnp.float32) * gate_scale_ref[...]
    up = jnp.dot(x, up_ref[...], preferred_element_type=jnp.float32) * up_scale_ref[...]
    hidden = (gate / (1.0 + jnp.exp(-gate)) * up).astype(jnp.bfloat16)
    term = product(hidden, down_ref[...])

    @pl.when(step == 0)
    def _():
        total[...] = term

    @pl.when(jnp.logical_and(step > 0, step < pl.num_programs(0) - 1))
    def _():
        total[...] += term

    @pl.when(step == pl.num_programs(0) - 1)
    def _():
        out_ref[...] = (total[...] + term).astype(jnp.bfloat16)


def mlp(inputs, gate_up, down_turned, gate_scale, up_scale):
    rows, width = inputs.shape
    units, tile = gate_scale.shape[0], 256
    tiles = units // tile
    return pl.pallas_call(
        mlp_kernel,
        grid=(tiles,),
        in_specs=[
            pl.BlockSpec((rows, width), lambda j: (0, 0)),
            pl.BlockSpec((width, tile), lambda j: (0, j)),
            pl.BlockSpec((width, tile), lambda j: (0, tiles + j)),
            pl.BlockSpec((width, tile), lambda j: (0, j)),
            pl.BlockSpec((1, tile), lambda j: (0, j)),
            pl.BlockSpec((1, tile), lambda j: (0, j)),
        ],
        out_specs=pl.BlockSpec((rows, width), lambda j: (0, 0)),
        out_shape=jax.ShapeDtypeStruct((rows, width), jnp.bfloat16),
        scratch_shapes=[pltpu.VMEM((rows, width), jnp.float32)],
        compiler_params=pltpu.CompilerParams(vmem_limit_bytes=62 * 1024 * 1024),
        cost_estimate=pl.CostEstimate(
            flops=6 * rows * width * units,
            bytes_accessed=6 * width * units + 4 * rows * width,
            transcendentals=rows * units,
        ),
    )(inputs, gate_up, gate_up, down_turned, gate_scale[None], up_scale[None])


def mixer_kernel(
    x_ref, weight_ref, scale_ref, cosine_ref, sine_ref, within_ref, fading_ref, rising_ref,
    decay_ref, out_ref, query, key, value, mixed,
):
    step = pl.program_id(0)

    def projected():
        return jnp.dot(x_ref[...], weight_ref[...], preferred_element_type=jnp.float32) * scale_ref[...]

    def turned():
        values = projected()
        half = values.shape[1] // 2
        a, b = values[:, :half], values[:, half:]
        cosine, sine = cosine_ref[...], sine_ref[...]
        return jnp.concatenate([a * cosine - b * sine, b * cosine + a * sine], axis=1)

    @pl.when(step == 0)
    def _():
        query[...] = turned().astype(jnp.bfloat16)

    @pl.when(step == 1)
    def _():
        key[...] = turned().astype(jnp.bfloat16)

    @pl.when(step == 2)
    def _():
        value[...] = projected().astype(jnp.bfloat16)
        blocks = query.shape[0] // BLOCK
        state = None
        for n in range(blocks):
            place = pl.ds(n * BLOCK, BLOCK)
            q, k, v = query[place, :], key[place, :], value[place, :]
            weights = (product(q, k) * within_ref[...]).astype(jnp.bfloat16)
            combined = jnp.dot(weights, v, preferred_element_type=jnp.float32)
            if n > 0:
                queried = q.astype(jnp.float32) * rising_ref[...]
                combined += jnp.dot(
                    queried, state, precision=HIGHEST, preferred_element_type=jnp.float32
                )
            if n < blocks - 1:
                faded = (k.astype(jnp.float32) * fading_ref[...]).T
                update = jnp.dot(
                    faded,
                    v.astype(jnp.float32),
                    precision=HIGHEST,
                    preferred_element_type=jnp.float32,
                )
                state = update if n == 0 else state * decay_ref[...] + update
            square = jnp.mean(combined * combined, axis=1, keepdims=True)
            normed = combined * lax.rsqrt(jnp.maximum(square, HEAD_FLOOR))
            mixed[place, :] = normed.astype(jnp.bfloat16)

    @pl.when(step == 3)
    def _():
        out_ref[...] = product(mixed[...], weight_ref[...]).astype(jnp.bfloat16)


def mixer(inputs, weights, scales, rate):
    rows, width = inputs.shape
    positions = jnp.arange(rows, dtype=jnp.float32)
    half = HEAD_DIM // 2
    frequency = ROTARY_BASE ** (-jnp.arange(half, dtype=jnp.float32) * 2.0 / HEAD_DIM)
    angles = positions[:, None] * frequency[None, :]
    inside = jnp.arange(BLOCK, dtype=jnp.float32)
    distance = inside[:, None] - inside[None, :]
    within = jnp.where(distance >= 0, jnp.exp(-rate * jnp.maximum(distance, 0.0)), 0.0)
    fading = jnp.exp(-rate * (BLOCK - 1.0 - inside[:, None])) * HEAD_DIM ** (-0.5)
    rising = jnp.exp(-rate * (inside[:, None] + 1.0))
    tables = (
        jnp.cos(angles),
        jnp.sin(angles),
        within * HEAD_DIM ** (-0.5),
        jnp.broadcast_to(fading, (BLOCK, HEAD_DIM)),
        jnp.broadcast_to(rising, (BLOCK, HEAD_DIM)),
        jnp.broadcast_to(jnp.exp(-rate * BLOCK), (1, HEAD_DIM)),
    )
    return pl.pallas_call(
        mixer_kernel,
        grid=(4,),
        in_specs=[
            pl.BlockSpec((rows, width), lambda j: (0, 0)),
            pl.BlockSpec((width, HEAD_DIM), lambda j: (0, j)),
            pl.BlockSpec((1, HEAD_DIM), lambda j: (0, jnp.minimum(j, 2))),
            *[pl.BlockSpec(t.shape, lambda j: (0, 0)) for t in tables],
        ],
        out_specs=pl.BlockSpec((rows, width), lambda j: (0, 0)),
        out_shape=jax.ShapeDtypeStruct((rows, width), jnp.bfloat16),
        scratch_shapes=[pltpu.VMEM((rows, HEAD_DIM), jnp.bfloat16) for _ in range(4)],
        compiler_params=pltpu.CompilerParams(vmem_limit_bytes=62 * 1024 * 1024),
        cost_estimate=pl.CostEstimate(
            flops=10 * rows * width * HEAD_DIM,
            bytes_accessed=8 * width * HEAD_DIM + 4 * rows * width,
            transcendentals=rows,
        ),
    )(inputs, weights, scales[None], *tables)


def body(
    residual_in,
    gain_first,
    gain_mixer,
    gain_second,
    gate_weight,
    gate_scale,
    up_weight,
    up_scale,
    down_weight,
    down_scale,
    query_weight,
    query_scale,
    key_weight,
    key_scale,
    value_weight,
    value_scale,
    output_weight,
    output_scale,
):
    low = jnp.bfloat16
    z, rows = lax.axis_size("z"), gate_weight.shape[0]
    hidden_width, local_width = down_weight.shape[0], query_weight.shape[1]
    first_part = jnp.concatenate([gate_weight.astype(low), up_weight.astype(low)], axis=1)
    second_part = scaled_columns(down_weight, down_scale)
    third_part = jnp.concatenate(
        [
            query_weight.astype(low),
            key_weight.astype(low),
            value_weight.astype(low),
            scaled_columns(output_weight, output_scale),
        ],
        axis=1,
    )
    first_y = lax.all_gather(first_part, "y", axis=0, tiled=True)
    first_full = lax.all_gather(first_y, "z", axis=0, tiled=True)
    second_z = lax.all_gather(after(second_part, first_y), "z", axis=0, tiled=True)
    second_near = y_neighbours(second_z)
    first_input = collect_rows(after(residual_in, second_z), gain_first)
    third_y = lax.all_gather(after(third_part, second_z), "y", axis=0, tiled=True)
    third_full = lax.all_gather(third_y, "z", axis=0, tiled=True)
    second_far = y_opposite(*second_near)
    down_full = joined_over_y(
        *[
            x.reshape(z, rows, hidden_width)
            for x in (second_z, *second_near, jnp.concatenate(second_far, axis=0))
        ]
    )

    def feed_forward(inputs):
        return summed_rows(mlp(inputs, first_full, down_full, gate_scale, up_scale))

    mlp_first = feed_forward(first_input)
    middle = (residual_in.astype(jnp.float32) + 0.5 * mlp_first).astype(low)
    scales = jnp.concatenate([query_scale, key_scale, value_scale])
    rate = head_rates(lax.axis_index("tp"), 1, TOK)[0]
    mixer_term = mixer(collect_rows(middle, gain_mixer), third_full, scales, rate)
    second = (middle.astype(jnp.float32) + summed_rows(mixer_term)).astype(low)
    mlp_second = feed_forward(collect_rows(second, gain_second))
    return (second.astype(jnp.float32) + 0.5 * mlp_second).astype(low)


def solution(mesh):
    split = Mesh(mesh.devices.reshape(16, 4, mesh.shape["tp"]), ("z", "y", "tp"))
    in_specs = (
        P(FS_TP, None),
        P(),
        P(),
        P(),
        P(FS, "tp"),
        P("tp"),
        P(FS, "tp"),
        P("tp"),
        P("tp", FS),
        P(FS),
        P(FS, "tp"),
        P("tp"),
        P(FS, "tp"),
        P("tp"),
        P(FS, "tp"),
        P("tp"),
        P("tp", FS),
        P(FS),
    )
    out_specs = P(FS_TP, None)
    return jax.shard_map(body, mesh=split, in_specs=in_specs, out_specs=out_specs, check_vma=False)
```

```python
import jax
import jax.numpy as jnp
from jax import lax
from jax.experimental import pallas as pl
from jax.experimental.pallas import tpu as pltpu
from jax.sharding import Mesh
from jax.sharding import PartitionSpec as P


HEADS = 8
HEAD_DIM = 256
BLOCK = 64
TOK = 256
FS = ("z", "y")
TP = ("x", "c")
FS_TP = ("z", "y", "x", "c")


EPSILON = 1e-06
HEAD_FLOOR = 0.25
ROTARY_BASE = 10000.0
HIGHEST = lax.Precision.HIGHEST


def spread(own_rows):
    peers = lax.axis_size("x")
    sent = jnp.broadcast_to(own_rows[None], (peers, *own_rows.shape))
    return lax.all_to_all(sent, "x", 0, 0, tiled=True).reshape(-1, own_rows.shape[1])


def swapped(x):
    return lax.ppermute(x, "c", [(0, 1), (1, 0)])


def shifted(x, axis, by):
    peers = lax.axis_size(axis)
    return lax.ppermute(x, axis, [(i, (i + by) % peers) for i in range(peers)])


def after(x, first):
    return lax.optimization_barrier((x, first))[0]


def y_neighbours(part):
    return shifted(part, "y", 1), shifted(part, "y", -1)


def y_opposite(below, above):
    half = below.shape[0] // 2
    return shifted(below[:half], "y", 1), shifted(above[half:], "y", -1)


def joined_over_y(part, below, above, far):
    me, peers = lax.axis_index("y"), lax.axis_size("y")
    own = part[:, :, None]
    whole = jnp.broadcast_to(own, (*part.shape[:2], peers, *part.shape[2:]))
    for piece, by in ((below, 3), (far, 2), (above, 1)):
        place = (0, 0, (me + by) % peers, 0, 0)
        whole = lax.dynamic_update_slice(whole, piece[:, :, None], place)
    return whole.reshape(part.shape[0], -1, part.shape[3])


def scaled_columns(weight, factor):
    low = weight.T.astype(jnp.bfloat16).astype(jnp.float32)
    return (low * factor[:, None]).astype(jnp.bfloat16)


def normalize(sequence_rows, gain_vector):
    values = sequence_rows.astype(jnp.float32)
    scaled = values * lax.rsqrt(jnp.mean(values * values, axis=-1, keepdims=True) + EPSILON)
    return (scaled * gain_vector).astype(jnp.bfloat16)


def collect_rows(own_rows, gain_vector):
    near = spread(normalize(own_rows, gain_vector))
    return near, swapped(near)


def product(inputs, turned):
    return lax.dot_general(
        inputs, turned, (((1,), (1,)), ((), ())), preferred_element_type=jnp.float32
    )


def return_rows(near, far):
    pair = near.astype(jnp.float32) + swapped(far).astype(jnp.float32)
    pieces = pair.astype(jnp.bfloat16).reshape(lax.axis_size("x"), -1, near.shape[1])
    arrived = lax.all_to_all(pieces, "x", 0, 0, tiled=True)
    return arrived.astype(jnp.float32).sum(axis=0)


def head_rates(first_head, head_count, length):
    head_number = (first_head + jnp.arange(head_count)).astype(jnp.float32)
    return jnp.exp(jnp.log(1.0 / 16.0) + head_number / (HEADS - 1) * jnp.log(4.0 / length))


def mlp_kernel(
    near_ref, far_ref, gate_ref, up_ref, down_ref, gate_scale_ref, up_scale_ref,
    out_near_ref, out_far_ref, both, total,
):
    step = pl.program_id(0)
    half = near_ref.shape[0]

    @pl.when(step == 0)
    def _():
        both[:half, :] = near_ref[...]
        both[half:, :] = far_ref[...]

    x = both[...]
    gate = jnp.dot(x, gate_ref[...], preferred_element_type=jnp.float32) * gate_scale_ref[...]
    up = jnp.dot(x, up_ref[...], preferred_element_type=jnp.float32) * up_scale_ref[...]
    hidden = (gate / (1.0 + jnp.exp(-gate)) * up).astype(jnp.bfloat16)
    term = product(hidden, down_ref[...])

    @pl.when(step == 0)
    def _():
        total[...] = term

    @pl.when(jnp.logical_and(step > 0, step < pl.num_programs(0) - 1))
    def _():
        total[...] += term

    @pl.when(step == pl.num_programs(0) - 1)
    def _():
        whole = (total[...] + term).astype(jnp.bfloat16)
        out_near_ref[...] = whole[:half, :]
        out_far_ref[...] = whole[half:, :]


def mlp(near, far, gate_up, down_turned, gate_scale, up_scale):
    half, width = near.shape
    rows = 2 * half
    units, tile = gate_scale.shape[0], 256
    tiles = units // tile
    return pl.pallas_call(
        mlp_kernel,
        grid=(tiles,),
        in_specs=[
            pl.BlockSpec((half, width), lambda j: (0, 0)),
            pl.BlockSpec((half, width), lambda j: (0, 0)),
            pl.BlockSpec((width, tile), lambda j: (0, j)),
            pl.BlockSpec((width, tile), lambda j: (0, tiles + j)),
            pl.BlockSpec((width, tile), lambda j: (0, j)),
            pl.BlockSpec((1, tile), lambda j: (0, j)),
            pl.BlockSpec((1, tile), lambda j: (0, j)),
        ],
        out_specs=[pl.BlockSpec((half, width), lambda j: (0, 0))] * 2,
        out_shape=[jax.ShapeDtypeStruct((half, width), jnp.bfloat16)] * 2,
        scratch_shapes=[
            pltpu.VMEM((rows, width), jnp.bfloat16),
            pltpu.VMEM((rows, width), jnp.float32),
        ],
        compiler_params=pltpu.CompilerParams(vmem_limit_bytes=62 * 1024 * 1024),
        cost_estimate=pl.CostEstimate(
            flops=6 * rows * width * units,
            bytes_accessed=6 * width * units + 4 * rows * width,
            transcendentals=rows * units,
        ),
    )(near, far, gate_up, gate_up, down_turned, gate_scale[None], up_scale[None])


def mixer_kernel(
    place_ref, near_ref, far_ref, own_ref, below_ref, above_ref, far_first_ref, far_second_ref, scale_ref,
    cosine_ref, sine_ref, within_ref, fading_ref, rising_ref, decay_ref, out_near_ref, out_far_ref,
    both, weight, query, key, value, mixed, sorted_,
):
    step = pl.program_id(0)
    half = near_ref.shape[0]
    rows = half // 4
    core, y = place_ref[0], place_ref[1]
    split = far_first_ref.shape[0]
    for piece_ref, by in ((own_ref, 0), (below_ref, 3), (above_ref, 1)):
        weight[:, lax.rem(y + by, 4), :, :] = piece_ref[:, 0]
    weight[:split, lax.rem(y + 2, 4), :, :] = far_first_ref[:, 0]
    weight[split:, lax.rem(y + 2, 4), :, :] = far_second_ref[:, 0]

    def whole_weight():
        return weight[...].reshape(-1, weight.shape[3])

    def place_of(part, number):
        return pl.ds(pl.multiple_of(part * 2 * rows + number * rows, rows), rows)

    @pl.when(step == 0)
    def _():
        for part in range(4):
            here = pl.ds(part * rows, rows)
            both[place_of(part, core), :] = near_ref[here, :]
            both[place_of(part, 1 - core), :] = far_ref[here, :]

    def projected():
        return jnp.dot(both[...], whole_weight(), preferred_element_type=jnp.float32) * scale_ref[...]

    def turned():
        values = projected()
        middle = values.shape[1] // 2
        a, b = values[:, :middle], values[:, middle:]
        cosine, sine = cosine_ref[...], sine_ref[...]
        return jnp.concatenate([a * cosine - b * sine, b * cosine + a * sine], axis=1)

    @pl.when(step == 0)
    def _():
        query[...] = turned().astype(jnp.bfloat16)

    @pl.when(step == 1)
    def _():
        key[...] = turned().astype(jnp.bfloat16)

    @pl.when(step == 2)
    def _():
        value[...] = projected().astype(jnp.bfloat16)
        blocks = query.shape[0] // BLOCK
        state = None
        for n in range(blocks):
            place = pl.ds(n * BLOCK, BLOCK)
            q, k, v = query[place, :], key[place, :], value[place, :]
            weights = (product(q, k) * within_ref[...]).astype(jnp.bfloat16)
            combined = jnp.dot(weights, v, preferred_element_type=jnp.float32)
            if n > 0:
                queried = q.astype(jnp.float32) * rising_ref[...]
                combined += jnp.dot(
                    queried, state, precision=HIGHEST, preferred_element_type=jnp.float32
                )
            if n < blocks - 1:
                faded = (k.astype(jnp.float32) * fading_ref[...]).T
                update = jnp.dot(
                    faded,
                    v.astype(jnp.float32),
                    precision=HIGHEST,
                    preferred_element_type=jnp.float32,
                )
                state = update if n == 0 else state * decay_ref[...] + update
            square = jnp.mean(combined * combined, axis=1, keepdims=True)
            normed = combined * lax.rsqrt(jnp.maximum(square, HEAD_FLOOR))
            mixed[place, :] = normed.astype(jnp.bfloat16)


    @pl.when(step == 3)
    def _():
        for part in range(4):
            here, there = pl.ds(part * rows, rows), pl.ds(half + part * rows, rows)
            sorted_[here, :] = mixed[place_of(part, core), :]
            sorted_[there, :] = mixed[place_of(part, 1 - core), :]
        whole = product(sorted_[...], whole_weight()).astype(jnp.bfloat16)
        out_near_ref[...] = whole[:half, :]
        out_far_ref[...] = whole[half:, :]


def mixer(near, far, pieces, scales, rate, core, y):
    half_rows, width = near.shape
    rows = 2 * half_rows
    positions = jnp.arange(rows, dtype=jnp.float32)
    half = HEAD_DIM // 2
    frequency = ROTARY_BASE ** (-jnp.arange(half, dtype=jnp.float32) * 2.0 / HEAD_DIM)
    angles = positions[:, None] * frequency[None, :]
    inside = jnp.arange(BLOCK, dtype=jnp.float32)
    distance = inside[:, None] - inside[None, :]
    within = jnp.where(distance >= 0, jnp.exp(-rate * jnp.maximum(distance, 0.0)), 0.0)
    fading = jnp.exp(-rate * (BLOCK - 1.0 - inside[:, None])) * HEAD_DIM ** (-0.5)
    rising = jnp.exp(-rate * (inside[:, None] + 1.0))
    tables = (
        jnp.cos(angles),
        jnp.sin(angles),
        within * HEAD_DIM ** (-0.5),
        jnp.broadcast_to(fading, (BLOCK, HEAD_DIM)),
        jnp.broadcast_to(rising, (BLOCK, HEAD_DIM)),
        jnp.broadcast_to(jnp.exp(-rate * BLOCK), (1, HEAD_DIM)),
    )
    return pl.pallas_call(
        mixer_kernel,
        grid=(4,),
        in_specs=[
            pl.BlockSpec(memory_space=pltpu.SMEM),
            pl.BlockSpec((half_rows, width), lambda j: (0, 0)),
            pl.BlockSpec((half_rows, width), lambda j: (0, 0)),
            *[
                pl.BlockSpec((x.shape[0], 1, *x.shape[2:]), lambda j: (0, j, 0, 0))
                for x in pieces
            ],
            pl.BlockSpec((1, HEAD_DIM), lambda j: (0, jnp.minimum(j, 2))),
            *[pl.BlockSpec(t.shape, lambda j: (0, 0)) for t in tables],
        ],
        out_specs=[pl.BlockSpec((half_rows, width), lambda j: (0, 0))] * 2,
        out_shape=[jax.ShapeDtypeStruct((half_rows, width), jnp.bfloat16)] * 2,
        scratch_shapes=[
            pltpu.VMEM((rows, width), jnp.bfloat16),
            pltpu.VMEM((pieces[0].shape[0], 4, *pieces[0].shape[2:]), jnp.bfloat16),
            *[pltpu.VMEM((rows, HEAD_DIM), jnp.bfloat16) for _ in range(5)],
        ],
        compiler_params=pltpu.CompilerParams(vmem_limit_bytes=62 * 1024 * 1024),
        cost_estimate=pl.CostEstimate(
            flops=10 * rows * width * HEAD_DIM,
            bytes_accessed=8 * width * HEAD_DIM + 4 * rows * width,
            transcendentals=rows,
        ),
    )(jnp.stack([core, y]).astype(jnp.int32), near, far, *pieces, scales[None], *tables)


def layer(
    residual_in,
    gain_first,
    gain_mixer,
    gain_second,
    gate_weight,
    gate_scale,
    up_weight,
    up_scale,
    down_weight,
    down_scale,
    query_weight,
    query_scale,
    key_weight,
    key_scale,
    value_weight,
    value_scale,
    output_weight,
    output_scale,
):
    low = jnp.bfloat16
    z, rows = lax.axis_size("z"), gate_weight.shape[0]
    hidden_width, local_width = down_weight.shape[0], query_weight.shape[1]
    first_part = jnp.concatenate([gate_weight.astype(low), up_weight.astype(low)], axis=1)
    second_part = scaled_columns(down_weight, down_scale)
    third_part = jnp.concatenate(
        [
            query_weight.astype(low),
            key_weight.astype(low),
            value_weight.astype(low),
            scaled_columns(output_weight, output_scale),
        ],
        axis=0,
    )
    packed = jnp.pad(first_part, ((0, 0), (0, local_width)))
    packed_y = lax.all_gather(packed, "y", axis=0, tiled=True)
    packed_y = lax.dynamic_update_slice(packed_y, third_part, (0, 2 * hidden_width))
    whole_z = lax.all_gather(packed_y, "z", axis=0, tiled=True)
    second_z = lax.all_gather(after(second_part, packed_y), "z", axis=0, tiled=True)
    second_near = y_neighbours(second_z)
    first_rows = collect_rows(after(residual_in, second_z), gain_first)
    second_far = y_opposite(*second_near)
    down_full = joined_over_y(
        *[
            x.reshape(1, z, rows, hidden_width)
            for x in (second_z, *second_near, jnp.concatenate(second_far, axis=0))
        ]
    )[0]
    third_z = whole_z[:, 2 * hidden_width :]
    third_below = shifted(third_z, "y", 1)
    third_above = shifted(third_z, "y", -1)
    half = third_z.shape[0] // 2
    far_first = shifted(third_below[:half], "y", 1)
    far_second = shifted(third_above[half:], "y", -1)
    first_term = mlp(*first_rows, whole_z, down_full, gate_scale, up_scale)
    mlp_first = return_rows(*first_term)
    pieces = [
        x.reshape(-1, 4, rows, local_width)
        for x in (third_z, third_below, third_above, far_first, far_second)
    ]
    middle = (residual_in.astype(jnp.float32) + 0.5 * mlp_first).astype(low)
    scales = jnp.concatenate([query_scale, key_scale, value_scale])
    core = lax.axis_index("c")
    rate = head_rates(lax.axis_index("x") * lax.axis_size("c") + core, 1, TOK)[0]
    mixer_rows = collect_rows(middle, gain_mixer)
    mixer_term = mixer(*mixer_rows, pieces, scales, rate, core, lax.axis_index("y"))
    second = (middle.astype(jnp.float32) + return_rows(*mixer_term)).astype(low)
    second_rows = collect_rows(second, gain_second)
    mlp_second = return_rows(*mlp(*second_rows, whole_z, down_full, gate_scale, up_scale))
    return (second.astype(jnp.float32) + 0.5 * mlp_second).astype(low)


def solution(mesh):
    split = Mesh(mesh.devices.reshape(16, 4, 4, 2), FS_TP)
    in_specs = (
        P(FS_TP, None),
        P(),
        P(),
        P(),
        P(FS, TP),
        P(TP),
        P(FS, TP),
        P(TP),
        P(TP, FS),
        P(FS),
        P(FS, TP),
        P(TP),
        P(FS, TP),
        P(TP),
        P(FS, TP),
        P(TP),
        P(TP, FS),
        P(FS),
    )
    out_specs = P(FS_TP, None)
    return jax.shard_map(layer, mesh=split, in_specs=in_specs, out_specs=out_specs, check_vma=False)
```

```python
import jax
import jax.numpy as jnp
from jax import lax
from jax.experimental import pallas as pl
from jax.experimental.pallas import tpu as pltpu
from jax.sharding import Mesh
from jax.sharding import PartitionSpec as P


HEADS = 8
HEAD_DIM = 256
BLOCK = 64
TOK = 256
FS = ("z", "y")
TP = ("x", "c")
FS_TP = ("z", "y", "x", "c")


EPSILON = 1e-06
HEAD_FLOOR = 0.25
ROTARY_BASE = 10000.0
HIGHEST = lax.Precision.HIGHEST


def spread(own_rows):
    peers = lax.axis_size("x")
    sent = jnp.broadcast_to(own_rows[None], (peers, *own_rows.shape))
    return lax.all_to_all(sent, "x", 0, 0, tiled=True).reshape(-1, own_rows.shape[1])


def swapped(x):
    return lax.ppermute(x, "c", [(0, 1), (1, 0)])


def shifted(x, axis, by):
    peers = lax.axis_size(axis)
    return lax.ppermute(x, axis, [(i, (i + by) % peers) for i in range(peers)])


def after(x, first):
    return lax.optimization_barrier((x, first))[0]


def y_neighbours(part):
    return shifted(part, "y", 1), shifted(part, "y", -1)


def y_opposite(below, above):
    half = below.shape[0] // 2
    return shifted(below[:half], "y", 1), shifted(above[half:], "y", -1)


def joined_over_y(part, below, above, far):
    me, peers = lax.axis_index("y"), lax.axis_size("y")
    own = part[:, :, None]
    whole = jnp.broadcast_to(own, (*part.shape[:2], peers, *part.shape[2:]))
    for piece, by in ((below, 3), (far, 2), (above, 1)):
        place = (0, 0, (me + by) % peers, 0, 0)
        whole = lax.dynamic_update_slice(whole, piece[:, :, None], place)
    return whole.reshape(part.shape[0], -1, part.shape[3])


def prepare_kernel(
    gate_ref, up_ref, down_ref, down_scale_ref, query_ref, key_ref, value_ref, output_ref, output_scale_ref,
    first_ref, second_ref, third_ref,
):
    low = jnp.bfloat16
    rows, hidden_width = gate_ref.shape
    width = query_ref.shape[1]
    first_ref[:, :hidden_width] = gate_ref[...].astype(low)
    first_ref[:, hidden_width : 2 * hidden_width] = up_ref[...].astype(low)
    first_ref[:, 2 * hidden_width :] = jnp.zeros((rows, width), low)
    second_ref[...] = scaled_rows(down_ref[...], down_scale_ref[...])
    for k, ref in enumerate((query_ref, key_ref, value_ref)):
        third_ref[pl.ds(k * rows, rows), :] = ref[...].astype(low)
    third_ref[pl.ds(3 * rows, rows), :] = scaled_rows(output_ref[...], output_scale_ref[...])


def scaled_rows(turned, factor):
    low = turned.astype(jnp.bfloat16).astype(jnp.float32)
    column = jnp.broadcast_to(factor, (8, factor.shape[1])).T[:, :1]
    return (low * column).astype(jnp.bfloat16)


def prepare(gate, up, down, down_scale, query, key, value, output, output_scale):
    rows, hidden_width = gate.shape
    width = query.shape[1]
    shapes = ((rows, 2 * hidden_width + width), (rows, hidden_width), (4 * rows, width))
    return pl.pallas_call(
        prepare_kernel,
        out_shape=[jax.ShapeDtypeStruct(x, jnp.bfloat16) for x in shapes],
        cost_estimate=pl.CostEstimate(
            flops=rows * (3 * hidden_width + 4 * width),
            bytes_accessed=6 * rows * (3 * hidden_width + 4 * width),
            transcendentals=0,
        ),
    )(
        gate, up, down.T, down_scale[None], query, key, value, output.T, output_scale[None]
    )


def normalize(sequence_rows, gain_vector):
    values = sequence_rows.astype(jnp.float32)
    scaled = values * lax.rsqrt(jnp.mean(values * values, axis=-1, keepdims=True) + EPSILON)
    return (scaled * gain_vector).astype(jnp.bfloat16)


def collect_rows(own_rows, gain_vector):
    near = spread(normalize(own_rows, gain_vector))
    return near, swapped(near)


def product(inputs, turned):
    return lax.dot_general(
        inputs, turned, (((1,), (1,)), ((), ())), preferred_element_type=jnp.float32
    )


def return_rows(near, far):
    pair = near.astype(jnp.float32) + swapped(far).astype(jnp.float32)
    pieces = pair.astype(jnp.bfloat16).reshape(lax.axis_size("x"), -1, near.shape[1])
    arrived = lax.all_to_all(pieces, "x", 0, 0, tiled=True)
    return arrived.astype(jnp.float32).sum(axis=0)


def head_rates(first_head, head_count, length):
    head_number = (first_head + jnp.arange(head_count)).astype(jnp.float32)
    return jnp.exp(jnp.log(1.0 / 16.0) + head_number / (HEADS - 1) * jnp.log(4.0 / length))


VMEM = pl.BlockSpec(memory_space=pltpu.VMEM)
KERNEL_PARAMS = pltpu.CompilerParams(vmem_limit_bytes=20 * 1024 * 1024)


def mlp_kernel(near_ref, far_ref, gate_up, down, gate_scale, up_scale, out_near, out_far):
    half, width = near_ref.shape
    units, tile = down.shape[1], 256
    x = jnp.concatenate([near_ref[...], far_ref[...]], axis=0)
    hidden = []
    for first in range(0, units, tile):
        here, there = pl.ds(first, tile), pl.ds(units + first, tile)
        gate = jnp.dot(x, gate_up[:, here], preferred_element_type=jnp.float32)
        up = jnp.dot(x, gate_up[:, there], preferred_element_type=jnp.float32)
        gate, up = gate * gate_scale[:, here], up * up_scale[:, here]
        hidden.append((gate / (1.0 + jnp.exp(-gate)) * up).astype(jnp.bfloat16))
    hidden = jnp.concatenate(hidden, axis=1)
    for first in range(0, width, 512):
        here = pl.ds(first, 512)
        term = product(hidden, down[here, :]).astype(jnp.bfloat16)
        out_near[:, here] = term[:half, :]
        out_far[:, here] = term[half:, :]


def mlp(near, far, gate_up, down_turned, gate_scale, up_scale):
    half, width = near.shape
    units = gate_scale.shape[0]
    return pl.pallas_call(
        mlp_kernel,
        in_specs=[VMEM] * 6,
        out_specs=[VMEM] * 2,
        out_shape=[jax.ShapeDtypeStruct((half, width), jnp.bfloat16)] * 2,
        compiler_params=KERNEL_PARAMS,
        cost_estimate=pl.CostEstimate(
            flops=12 * half * width * units,
            bytes_accessed=6 * width * units + 8 * half * width,
            transcendentals=2 * half * units,
        ),
    )(near, far, gate_up, down_turned, gate_scale[None], up_scale[None])


def mixer_kernel(
    place_ref, near_ref, far_ref, own_ref, below_ref, above_ref, beyond_ref, scale_ref,
    cosine_ref, sine_ref, within_ref, fading_ref, rising_ref, decay_ref, out_near_ref, out_far_ref,
    both, weight, query, key, value, mixed, sorted_,
):
    half = near_ref.shape[0]
    rows = half // 4
    core, y = place_ref[0], place_ref[1]

    def place_of(part, number):
        return pl.ds(pl.multiple_of(part * 2 * rows + number * rows, rows), rows)

    def whole_weight(k):
        for piece_ref, by in ((own_ref, 0), (below_ref, 3), (above_ref, 1), (beyond_ref, 2)):
            weight[k, :, lax.rem(y + by, 4), :, :] = piece_ref[:, k]
        return weight[k].reshape(-1, HEAD_DIM)

    for part in range(4):
        here = pl.ds(part * rows, rows)
        both[place_of(part, core), :] = near_ref[here, :]
        both[place_of(part, 1 - core), :] = far_ref[here, :]

    def projected(k):
        pre = jnp.dot(both[...], whole_weight(k), preferred_element_type=jnp.float32)
        return pre * scale_ref[:, k * HEAD_DIM : (k + 1) * HEAD_DIM]

    def turned(values):
        middle = HEAD_DIM // 2
        a, b = values[:, :middle], values[:, middle:]
        cosine, sine = cosine_ref[...], sine_ref[...]
        return jnp.concatenate([a * cosine - b * sine, b * cosine + a * sine], axis=1)

    query[...] = turned(projected(0)).astype(jnp.bfloat16)
    key[...] = turned(projected(1)).astype(jnp.bfloat16)
    value[...] = projected(2).astype(jnp.bfloat16)
    blocks = query.shape[0] // BLOCK
    state = None
    for n in range(blocks):
        place = pl.ds(n * BLOCK, BLOCK)
        q, k, v = query[place, :], key[place, :], value[place, :]
        weights = (product(q, k) * within_ref[...]).astype(jnp.bfloat16)
        combined = jnp.dot(weights, v, preferred_element_type=jnp.float32)
        if n > 0:
            queried = q.astype(jnp.float32) * rising_ref[...]
            combined += jnp.dot(
                queried, state, precision=HIGHEST, preferred_element_type=jnp.float32
            )
        if n < blocks - 1:
            faded = (k.astype(jnp.float32) * fading_ref[...]).T
            update = jnp.dot(
                faded,
                v.astype(jnp.float32),
                precision=HIGHEST,
                preferred_element_type=jnp.float32,
            )
            state = update if n == 0 else state * decay_ref[...] + update
        square = jnp.mean(combined * combined, axis=1, keepdims=True)
        normed = combined * lax.rsqrt(jnp.maximum(square, HEAD_FLOOR))
        mixed[place, :] = normed.astype(jnp.bfloat16)
    for part in range(4):
        here, there = pl.ds(part * rows, rows), pl.ds(half + part * rows, rows)
        sorted_[here, :] = mixed[place_of(part, core), :]
        sorted_[there, :] = mixed[place_of(part, 1 - core), :]
    output = whole_weight(3)
    for first in range(0, output.shape[0], 512):
        here = pl.ds(first, 512)
        term = product(sorted_[...], output[first : first + 512, :]).astype(jnp.bfloat16)
        out_near_ref[:, here] = term[:half, :]
        out_far_ref[:, here] = term[half:, :]


def mixer_tables(rows, rate):
    positions = jnp.arange(rows, dtype=jnp.float32)
    half = HEAD_DIM // 2
    frequency = ROTARY_BASE ** (-jnp.arange(half, dtype=jnp.float32) * 2.0 / HEAD_DIM)
    angles = positions[:, None] * frequency[None, :]
    inside = jnp.arange(BLOCK, dtype=jnp.float32)
    distance = inside[:, None] - inside[None, :]
    within = jnp.where(distance >= 0, jnp.exp(-rate * jnp.maximum(distance, 0.0)), 0.0)
    fading = jnp.exp(-rate * (BLOCK - 1.0 - inside[:, None])) * HEAD_DIM ** (-0.5)
    rising = jnp.exp(-rate * (inside[:, None] + 1.0))
    return (
        jnp.cos(angles),
        jnp.sin(angles),
        within * HEAD_DIM ** (-0.5),
        jnp.broadcast_to(fading, (BLOCK, HEAD_DIM)),
        jnp.broadcast_to(rising, (BLOCK, HEAD_DIM)),
        jnp.broadcast_to(jnp.exp(-rate * BLOCK), (1, HEAD_DIM)),
    )


def mixer(near, far, pieces, scales, tables, place):
    half_rows, width = near.shape
    rows = 2 * half_rows
    return pl.pallas_call(
        mixer_kernel,
        in_specs=[
            pl.BlockSpec(memory_space=pltpu.SMEM),
            *[VMEM] * (3 + len(pieces) + len(tables)),
        ],
        out_specs=[VMEM] * 2,
        out_shape=[jax.ShapeDtypeStruct((half_rows, width), jnp.bfloat16)] * 2,
        scratch_shapes=[
            pltpu.VMEM((rows, width), jnp.bfloat16),
            pltpu.VMEM((4, pieces[0].shape[0], 4, *pieces[0].shape[2:]), jnp.bfloat16),
            *[pltpu.VMEM((rows, HEAD_DIM), jnp.bfloat16) for _ in range(5)],
        ],
        compiler_params=KERNEL_PARAMS,
        cost_estimate=pl.CostEstimate(
            flops=10 * rows * width * HEAD_DIM,
            bytes_accessed=8 * width * HEAD_DIM + 4 * rows * width,
            transcendentals=rows,
        ),
    )(place, near, far, *pieces, scales[None], *tables)


def layer(
    residual_in,
    gain_first,
    gain_mixer,
    gain_second,
    gate_weight,
    gate_scale,
    up_weight,
    up_scale,
    down_weight,
    down_scale,
    query_weight,
    query_scale,
    key_weight,
    key_scale,
    value_weight,
    value_scale,
    output_weight,
    output_scale,
):
    low = jnp.bfloat16
    z, rows = lax.axis_size("z"), gate_weight.shape[0]
    hidden_width, local_width = down_weight.shape[0], query_weight.shape[1]
    packed, second_part, third_part = prepare(
        gate_weight, up_weight, down_weight, down_scale, query_weight, key_weight, value_weight,
        output_weight, output_scale,
    )
    packed_y = lax.all_gather(packed, "y", axis=0, tiled=True)
    packed_y = lax.dynamic_update_slice(packed_y, third_part, (0, 2 * hidden_width))
    whole_z = lax.all_gather(packed_y, "z", axis=0, tiled=True)
    second_z = lax.all_gather(after(second_part, packed_y), "z", axis=0, tiled=True)
    second_near = y_neighbours(second_z)
    first_rows = collect_rows(after(residual_in, second_z), gain_first)
    second_far = y_opposite(*second_near)
    down_full = joined_over_y(
        *[
            x.reshape(1, z, rows, hidden_width)
            for x in (second_z, *second_near, jnp.concatenate(second_far, axis=0))
        ]
    )[0]
    third_z = whole_z[:, 2 * hidden_width :]
    third_below = shifted(third_z, "y", 1)
    third_above = shifted(third_z, "y", -1)
    third_far = shifted(third_below, "y", 1)
    core = lax.axis_index("c")
    rate = head_rates(lax.axis_index("x") * lax.axis_size("c") + core, 1, TOK)[0]
    scales = jnp.concatenate([query_scale, key_scale, value_scale])
    place = jnp.stack([core, lax.axis_index("y")]).astype(jnp.int32)
    first_rows, scales, place = lax.optimization_barrier((first_rows, scales, place))
    first_term = mlp(*first_rows, whole_z, down_full, gate_scale, up_scale)
    tables = mixer_tables(TOK, rate)
    mlp_first = return_rows(*first_term)
    pieces = [
        x.reshape(-1, 4, rows, local_width)
        for x in (third_z, third_below, third_above, third_far)
    ]
    middle = (residual_in.astype(jnp.float32) + 0.5 * mlp_first).astype(low)
    mixer_rows = collect_rows(middle, gain_mixer)
    mixer_term = mixer(*mixer_rows, pieces, scales, tables, place)
    second = (middle.astype(jnp.float32) + return_rows(*mixer_term)).astype(low)
    second_rows = collect_rows(second, gain_second)
    mlp_second = return_rows(*mlp(*second_rows, whole_z, down_full, gate_scale, up_scale))
    return (second.astype(jnp.float32) + 0.5 * mlp_second).astype(low)


def solution(mesh):
    split = Mesh(mesh.devices.reshape(16, 4, 4, 2), FS_TP)
    in_specs = (
        P(FS_TP, None),
        P(),
        P(),
        P(),
        P(FS, TP),
        P(TP),
        P(FS, TP),
        P(TP),
        P(TP, FS),
        P(FS),
        P(FS, TP),
        P(TP),
        P(FS, TP),
        P(TP),
        P(FS, TP),
        P(TP),
        P(TP, FS),
        P(FS),
    )
    out_specs = P(FS_TP, None)
    return jax.shard_map(layer, mesh=split, in_specs=in_specs, out_specs=out_specs, check_vma=False)
```

```python
import jax
import jax.numpy as jnp
from jax import lax
from jax.experimental import pallas as pl
from jax.experimental.pallas import tpu as pltpu
from jax.sharding import Mesh
from jax.sharding import PartitionSpec as P


HEADS = 8
HEAD_DIM = 256
BLOCK = 64
TOK = 256
MOVED = 128
FS = ("z", "y")
TP = ("x", "c")
FS_TP = ("z", "y", "x", "c")


EPSILON = 1e-06
HEAD_FLOOR = 0.25
ROTARY_BASE = 10000.0
HIGHEST = lax.Precision.HIGHEST


def spread(own_rows):
    peers = lax.axis_size("x")
    sent = jnp.broadcast_to(own_rows[None], (peers, *own_rows.shape))
    return lax.all_to_all(sent, "x", 0, 0, tiled=True).reshape(-1, own_rows.shape[1])


def swapped(x):
    return lax.ppermute(x, "c", [(0, 1), (1, 0)])


def shifted(x, axis, by):
    peers = lax.axis_size(axis)
    return lax.ppermute(x, axis, [(i, (i + by) % peers) for i in range(peers)])


def after(x, first):
    return lax.optimization_barrier((x, first))[0]


def y_neighbours(part):
    return shifted(part, "y", 1), shifted(part, "y", -1)


def y_opposite(below, above):
    half = below.shape[0] // 2
    return shifted(below[:half], "y", 1), shifted(above[half:], "y", -1)


def joined_over_y(part, below, above, far):
    me, peers = lax.axis_index("y"), lax.axis_size("y")
    own = part[:, :, None]
    whole = jnp.broadcast_to(own, (*part.shape[:2], peers, *part.shape[2:]))
    for piece, by in ((below, 3), (far, 2), (above, 1)):
        place = (0, 0, (me + by) % peers, 0, 0)
        whole = lax.dynamic_update_slice(whole, piece[:, :, None], place)
    return whole.reshape(part.shape[0], -1, part.shape[3])


def prepare_kernel(
    gate_ref, up_ref, down_ref, down_scale_ref, query_ref, key_ref, value_ref, output_ref, output_scale_ref,
    first_ref, second_ref, third_ref,
):
    low = jnp.bfloat16
    rows, units = gate_ref.shape
    width = query_ref.shape[1]
    kept = units - MOVED
    first_ref[:, :units] = gate_ref[...].astype(low)
    first_ref[:, units : units + kept] = up_ref[:, :kept].astype(low)
    first_ref[:, units + kept :] = jnp.zeros((rows, width), low)
    second_ref[:, :units] = scaled_rows(down_ref[...], down_scale_ref[...])
    second_ref[:, units:] = up_ref[:, kept:].astype(low)
    for k, ref in enumerate((query_ref, key_ref, value_ref)):
        third_ref[pl.ds(k * rows, rows), :] = ref[...].astype(low)
    third_ref[pl.ds(3 * rows, rows), :] = scaled_rows(output_ref[...], output_scale_ref[...])


def scaled_rows(turned, factor):
    low = turned.astype(jnp.bfloat16).astype(jnp.float32)
    column = jnp.broadcast_to(factor, (8, factor.shape[1])).T[:, :1]
    return (low * column).astype(jnp.bfloat16)


def prepare(gate, up, down, down_scale, query, key, value, output, output_scale):
    rows, hidden_width = gate.shape
    width = query.shape[1]
    units = hidden_width
    shapes = ((rows, 2 * units - MOVED + width), (rows, units + MOVED), (4 * rows, width))
    return pl.pallas_call(
        prepare_kernel,
        out_shape=[jax.ShapeDtypeStruct(x, jnp.bfloat16) for x in shapes],
        cost_estimate=pl.CostEstimate(
            flops=rows * (3 * hidden_width + 4 * width),
            bytes_accessed=6 * rows * (3 * hidden_width + 4 * width),
            transcendentals=0,
        ),
    )(
        gate, up, down.T, down_scale[None], query, key, value, output.T, output_scale[None]
    )


def normalize(sequence_rows, gain_vector):
    values = sequence_rows.astype(jnp.float32)
    scaled = values * lax.rsqrt(jnp.mean(values * values, axis=-1, keepdims=True) + EPSILON)
    return (scaled * gain_vector).astype(jnp.bfloat16)


def collect_rows(own_rows, gain_vector):
    near = spread(normalize(own_rows, gain_vector))
    return near, swapped(near)


def product(inputs, turned):
    return lax.dot_general(
        inputs, turned, (((1,), (1,)), ((), ())), preferred_element_type=jnp.float32
    )


def return_rows(near, far):
    pair = near.astype(jnp.float32) + swapped(far).astype(jnp.float32)
    pieces = pair.astype(jnp.bfloat16).reshape(lax.axis_size("x"), -1, near.shape[1])
    arrived = lax.all_to_all(pieces, "x", 0, 0, tiled=True)
    return arrived.astype(jnp.float32).sum(axis=0)


def head_rates(first_head, head_count, length):
    head_number = (first_head + jnp.arange(head_count)).astype(jnp.float32)
    return jnp.exp(jnp.log(1.0 / 16.0) + head_number / (HEADS - 1) * jnp.log(4.0 / length))


VMEM = pl.BlockSpec(memory_space=pltpu.VMEM)
KERNEL_PARAMS = pltpu.CompilerParams(vmem_limit_bytes=20 * 1024 * 1024)


def mlp_kernel(near_ref, far_ref, gate_up, down, gate_scale, up_scale, out_near, out_far):
    half, width = near_ref.shape
    units, tile = down.shape[1] - MOVED, 256
    kept = units - MOVED
    x = jnp.concatenate([near_ref[...], far_ref[...]], axis=0)
    hidden = []
    for first in range(0, units, tile):
        here, there = pl.ds(first, tile), pl.ds(units + first, tile)
        gate = jnp.dot(x, gate_up[:, here], preferred_element_type=jnp.float32)
        if first + tile <= kept:
            up = jnp.dot(x, gate_up[:, there], preferred_element_type=jnp.float32)
        else:
            there = pl.ds(units + first, kept - first)
            up = [
                jnp.dot(x, w, preferred_element_type=jnp.float32)
                for w in (gate_up[:, there], down[:, units:])
            ]
            up = jnp.concatenate(up, axis=1)
        gate, up = gate * gate_scale[:, here], up * up_scale[:, here]
        hidden.append((gate / (1.0 + jnp.exp(-gate)) * up).astype(jnp.bfloat16))
    hidden = jnp.concatenate(hidden, axis=1)
    for first in range(0, width, 512):
        here = pl.ds(first, 512)
        term = product(hidden, down[here, :units]).astype(jnp.bfloat16)
        out_near[:, here] = term[:half, :]
        out_far[:, here] = term[half:, :]


def mlp(near, far, gate_up, down_turned, gate_scale, up_scale):
    half, width = near.shape
    units = gate_scale.shape[0]
    return pl.pallas_call(
        mlp_kernel,
        in_specs=[VMEM] * 6,
        out_specs=[VMEM] * 2,
        out_shape=[jax.ShapeDtypeStruct((half, width), jnp.bfloat16)] * 2,
        compiler_params=KERNEL_PARAMS,
        cost_estimate=pl.CostEstimate(
            flops=12 * half * width * units,
            bytes_accessed=6 * width * units + 8 * half * width,
            transcendentals=2 * half * units,
        ),
    )(near, far, gate_up, down_turned, gate_scale[None], up_scale[None])


def mixer_kernel(
    place_ref, near_ref, far_ref, own_ref, below_ref, above_ref, beyond_ref, scale_ref,
    cosine_ref, sine_ref, within_ref, fading_ref, rising_ref, decay_ref, out_near_ref, out_far_ref,
    both, weight, query, key, value, mixed, sorted_,
):
    half = near_ref.shape[0]
    rows = half // 4
    core, y = place_ref[0], place_ref[1]

    def place_of(part, number):
        return pl.ds(pl.multiple_of(part * 2 * rows + number * rows, rows), rows)

    def whole_weight(k):
        for piece_ref, by in ((own_ref, 0), (below_ref, 3), (above_ref, 1), (beyond_ref, 2)):
            weight[k, :, lax.rem(y + by, 4), :, :] = piece_ref[:, k]
        return weight[k].reshape(-1, HEAD_DIM)

    for part in range(4):
        here = pl.ds(part * rows, rows)
        both[place_of(part, core), :] = near_ref[here, :]
        both[place_of(part, 1 - core), :] = far_ref[here, :]

    def projected(k):
        pre = jnp.dot(both[...], whole_weight(k), preferred_element_type=jnp.float32)
        return pre * scale_ref[:, k * HEAD_DIM : (k + 1) * HEAD_DIM]

    def turned(values):
        middle = HEAD_DIM // 2
        a, b = values[:, :middle], values[:, middle:]
        cosine, sine = cosine_ref[...], sine_ref[...]
        return jnp.concatenate([a * cosine - b * sine, b * cosine + a * sine], axis=1)

    query[...] = turned(projected(0)).astype(jnp.bfloat16)
    key[...] = turned(projected(1)).astype(jnp.bfloat16)
    value[...] = projected(2).astype(jnp.bfloat16)
    blocks = query.shape[0] // BLOCK
    state = None
    for n in range(blocks):
        place = pl.ds(n * BLOCK, BLOCK)
        q, k, v = query[place, :], key[place, :], value[place, :]
        weights = (product(q, k) * within_ref[...]).astype(jnp.bfloat16)
        combined = jnp.dot(weights, v, preferred_element_type=jnp.float32)
        if n > 0:
            queried = q.astype(jnp.float32) * rising_ref[...]
            combined += jnp.dot(
                queried, state, precision=HIGHEST, preferred_element_type=jnp.float32
            )
        if n < blocks - 1:
            faded = (k.astype(jnp.float32) * fading_ref[...]).T
            update = jnp.dot(
                faded,
                v.astype(jnp.float32),
                precision=HIGHEST,
                preferred_element_type=jnp.float32,
            )
            state = update if n == 0 else state * decay_ref[...] + update
        square = jnp.mean(combined * combined, axis=1, keepdims=True)
        normed = combined * lax.rsqrt(jnp.maximum(square, HEAD_FLOOR))
        mixed[place, :] = normed.astype(jnp.bfloat16)
    for part in range(4):
        here, there = pl.ds(part * rows, rows), pl.ds(half + part * rows, rows)
        sorted_[here, :] = mixed[place_of(part, core), :]
        sorted_[there, :] = mixed[place_of(part, 1 - core), :]
    output = whole_weight(3)
    for first in range(0, output.shape[0], 512):
        here = pl.ds(first, 512)
        term = product(sorted_[...], output[first : first + 512, :]).astype(jnp.bfloat16)
        out_near_ref[:, here] = term[:half, :]
        out_far_ref[:, here] = term[half:, :]


def mixer_tables(rows, rate):
    positions = jnp.arange(rows, dtype=jnp.float32)
    half = HEAD_DIM // 2
    frequency = ROTARY_BASE ** (-jnp.arange(half, dtype=jnp.float32) * 2.0 / HEAD_DIM)
    angles = positions[:, None] * frequency[None, :]
    inside = jnp.arange(BLOCK, dtype=jnp.float32)
    distance = inside[:, None] - inside[None, :]
    within = jnp.where(distance >= 0, jnp.exp(-rate * jnp.maximum(distance, 0.0)), 0.0)
    fading = jnp.exp(-rate * (BLOCK - 1.0 - inside[:, None])) * HEAD_DIM ** (-0.5)
    rising = jnp.exp(-rate * (inside[:, None] + 1.0))
    return (
        jnp.cos(angles),
        jnp.sin(angles),
        within * HEAD_DIM ** (-0.5),
        jnp.broadcast_to(fading, (BLOCK, HEAD_DIM)),
        jnp.broadcast_to(rising, (BLOCK, HEAD_DIM)),
        jnp.broadcast_to(jnp.exp(-rate * BLOCK), (1, HEAD_DIM)),
    )


def mixer(near, far, pieces, scales, tables, place):
    half_rows, width = near.shape
    rows = 2 * half_rows
    return pl.pallas_call(
        mixer_kernel,
        in_specs=[
            pl.BlockSpec(memory_space=pltpu.SMEM),
            *[VMEM] * (3 + len(pieces) + len(tables)),
        ],
        out_specs=[VMEM] * 2,
        out_shape=[jax.ShapeDtypeStruct((half_rows, width), jnp.bfloat16)] * 2,
        scratch_shapes=[
            pltpu.VMEM((rows, width), jnp.bfloat16),
            pltpu.VMEM((4, pieces[0].shape[0], 4, *pieces[0].shape[2:]), jnp.bfloat16),
            *[pltpu.VMEM((rows, HEAD_DIM), jnp.bfloat16) for _ in range(5)],
        ],
        compiler_params=KERNEL_PARAMS,
        cost_estimate=pl.CostEstimate(
            flops=10 * rows * width * HEAD_DIM,
            bytes_accessed=8 * width * HEAD_DIM + 4 * rows * width,
            transcendentals=rows,
        ),
    )(place, near, far, *pieces, scales[None], *tables)


def layer(
    residual_in,
    gain_first,
    gain_mixer,
    gain_second,
    gate_weight,
    gate_scale,
    up_weight,
    up_scale,
    down_weight,
    down_scale,
    query_weight,
    query_scale,
    key_weight,
    key_scale,
    value_weight,
    value_scale,
    output_weight,
    output_scale,
):
    low = jnp.bfloat16
    z, rows = lax.axis_size("z"), gate_weight.shape[0]
    hidden_width, local_width = down_weight.shape[0], query_weight.shape[1]
    first_width = 2 * hidden_width - MOVED
    packed, second_part, third_part = prepare(
        gate_weight, up_weight, down_weight, down_scale, query_weight, key_weight, value_weight,
        output_weight, output_scale,
    )
    packed_y = lax.all_gather(packed, "y", axis=0, tiled=True)
    packed_y = lax.dynamic_update_slice(packed_y, third_part, (0, first_width))
    whole_z = lax.all_gather(packed_y, "z", axis=0, tiled=True)
    second_z = lax.all_gather(after(second_part, packed_y), "z", axis=0, tiled=True)
    second_near = y_neighbours(second_z)
    first_rows = collect_rows(after(residual_in, second_z), gain_first)
    second_far = y_opposite(*second_near)
    down_full = joined_over_y(
        *[
            x.reshape(1, z, rows, hidden_width + MOVED)
            for x in (second_z, *second_near, jnp.concatenate(second_far, axis=0))
        ]
    )[0]
    third_z = whole_z[:, first_width:]
    third_below = shifted(third_z, "y", 1)
    third_above = shifted(third_z, "y", -1)
    third_far = shifted(third_below, "y", 1)
    core = lax.axis_index("c")
    rate = head_rates(lax.axis_index("x") * lax.axis_size("c") + core, 1, TOK)[0]
    scales = jnp.concatenate([query_scale, key_scale, value_scale])
    place = jnp.stack([core, lax.axis_index("y")]).astype(jnp.int32)
    first_rows, scales, place = lax.optimization_barrier((first_rows, scales, place))
    first_term = mlp(*first_rows, whole_z, down_full, gate_scale, up_scale)
    tables = mixer_tables(TOK, rate)
    mlp_first = return_rows(*first_term)
    pieces = [
        x.reshape(-1, 4, rows, local_width)
        for x in (third_z, third_below, third_above, third_far)
    ]
    middle = (residual_in.astype(jnp.float32) + 0.5 * mlp_first).astype(low)
    mixer_rows = collect_rows(middle, gain_mixer)
    mixer_term = mixer(*mixer_rows, pieces, scales, tables, place)
    second = (middle.astype(jnp.float32) + return_rows(*mixer_term)).astype(low)
    second_rows = collect_rows(second, gain_second)
    mlp_second = return_rows(*mlp(*second_rows, whole_z, down_full, gate_scale, up_scale))
    return (second.astype(jnp.float32) + 0.5 * mlp_second).astype(low)


def solution(mesh):
    split = Mesh(mesh.devices.reshape(16, 4, 4, 2), FS_TP)
    in_specs = (
        P(FS_TP, None),
        P(),
        P(),
        P(),
        P(FS, TP),
        P(TP),
        P(FS, TP),
        P(TP),
        P(TP, FS),
        P(FS),
        P(FS, TP),
        P(TP),
        P(FS, TP),
        P(TP),
        P(FS, TP),
        P(TP),
        P(TP, FS),
        P(FS),
    )
    out_specs = P(FS_TP, None)
    return jax.shard_map(layer, mesh=split, in_specs=in_specs, out_specs=out_specs, check_vma=False)
```

```python
import jax
import jax.numpy as jnp
from jax import lax
from jax.experimental import pallas as pl
from jax.experimental.pallas import tpu as pltpu
from jax.sharding import Mesh
from jax.sharding import PartitionSpec as P


HEADS = 8
HEAD_DIM = 256
BLOCK = 64
TOK = 256
MOVED = 128
FS = ("z", "y")
TP = ("x", "c")
FS_TP = ("z", "y", "x", "c")


EPSILON = 1e-06
HEAD_FLOOR = 0.25
ROTARY_BASE = 10000.0
HIGHEST = lax.Precision.HIGHEST


def spread(own_rows):
    peers = lax.axis_size("x")
    sent = jnp.broadcast_to(own_rows[None], (peers, *own_rows.shape))
    return lax.all_to_all(sent, "x", 0, 0, tiled=True).reshape(-1, own_rows.shape[1])


def swapped(x):
    return lax.ppermute(x, "c", [(0, 1), (1, 0)])


def shifted(x, axis, by):
    peers = lax.axis_size(axis)
    return lax.ppermute(x, axis, [(i, (i + by) % peers) for i in range(peers)])


def after(x, first):
    return lax.optimization_barrier((x, first))[0]


def y_neighbours(part):
    return shifted(part, "y", 1), shifted(part, "y", -1)


def y_opposite(below, above):
    half = below.shape[0] // 2
    return shifted(below[:half], "y", 1), shifted(above[half:], "y", -1)


def joined_over_y(part, below, above, far):
    me, peers = lax.axis_index("y"), lax.axis_size("y")
    own = part[:, :, None]
    whole = jnp.broadcast_to(own, (*part.shape[:2], peers, *part.shape[2:]))
    for piece, by in ((below, 3), (far, 2), (above, 1)):
        place = (0, 0, (me + by) % peers, 0, 0)
        whole = lax.dynamic_update_slice(whole, piece[:, :, None], place)
    return whole.reshape(part.shape[0], -1, part.shape[3])


def prepare_kernel(
    gate_ref, up_ref, down_ref, down_scale_ref, query_ref, key_ref, value_ref, output_ref, output_scale_ref,
    first_ref, second_ref, third_ref,
):
    low = jnp.bfloat16
    rows, units = gate_ref.shape
    width = query_ref.shape[1]
    kept = units - MOVED
    for copy in range(first_ref.shape[0]):
        first_ref[copy, :, :units] = gate_ref[...].astype(low)
        first_ref[copy, :, units : units + kept] = up_ref[:, :kept].astype(low)
        first_ref[copy, :, units + kept :] = jnp.zeros((rows, width), low)
    second_ref[:, :units] = scaled_rows(down_ref[...], down_scale_ref[...])
    second_ref[:, units:] = up_ref[:, kept:].astype(low)
    for k, ref in enumerate((query_ref, key_ref, value_ref)):
        third_ref[pl.ds(k * rows, rows), :] = ref[...].astype(low)
    third_ref[pl.ds(3 * rows, rows), :] = scaled_rows(output_ref[...], output_scale_ref[...])


def scaled_rows(turned, factor):
    low = turned.astype(jnp.bfloat16).astype(jnp.float32)
    column = jnp.broadcast_to(factor, (8, factor.shape[1])).T[:, :1]
    return (low * column).astype(jnp.bfloat16)


def prepare(gate, up, down, down_scale, query, key, value, output, output_scale):
    rows, hidden_width = gate.shape
    width = query.shape[1]
    units = hidden_width
    first = (lax.axis_size("y"), rows, 2 * units - MOVED + width)
    shapes = (first, (rows, units + MOVED), (4 * rows, width))
    return pl.pallas_call(
        prepare_kernel,
        out_shape=[jax.ShapeDtypeStruct(x, jnp.bfloat16) for x in shapes],
        cost_estimate=pl.CostEstimate(
            flops=rows * (3 * hidden_width + 4 * width),
            bytes_accessed=6 * rows * (3 * hidden_width + 4 * width),
            transcendentals=0,
        ),
    )(
        gate, up, down.T, down_scale[None], query, key, value, output.T, output_scale[None]
    )


def normalize(sequence_rows, gain_vector):
    values = sequence_rows.astype(jnp.float32)
    scaled = values * lax.rsqrt(jnp.mean(values * values, axis=-1, keepdims=True) + EPSILON)
    return (scaled * gain_vector).astype(jnp.bfloat16)


def collect_rows(own_rows, gain_vector):
    near = spread(normalize(own_rows, gain_vector))
    return near, swapped(near)


def product(inputs, turned):
    return lax.dot_general(
        inputs, turned, (((1,), (1,)), ((), ())), preferred_element_type=jnp.float32
    )


def return_rows(near, far):
    pair = near.astype(jnp.float32) + swapped(far).astype(jnp.float32)
    pieces = pair.astype(jnp.bfloat16).reshape(lax.axis_size("x"), -1, near.shape[1])
    arrived = lax.all_to_all(pieces, "x", 0, 0, tiled=True)
    return arrived.astype(jnp.float32).sum(axis=0)


def head_rates(first_head, head_count, length):
    head_number = (first_head + jnp.arange(head_count)).astype(jnp.float32)
    return jnp.exp(jnp.log(1.0 / 16.0) + head_number / (HEADS - 1) * jnp.log(4.0 / length))


VMEM = pl.BlockSpec(memory_space=pltpu.VMEM)
KERNEL_PARAMS = pltpu.CompilerParams(vmem_limit_bytes=20 * 1024 * 1024)


def mlp_kernel(near_ref, far_ref, gate_up, down, gate_scale, up_scale, out_near, out_far):
    half, width = near_ref.shape
    units, tile = down.shape[1] - MOVED, 256
    kept = units - MOVED
    x = jnp.concatenate([near_ref[...], far_ref[...]], axis=0)
    hidden = []
    for first in range(0, units, tile):
        here, there = pl.ds(first, tile), pl.ds(units + first, tile)
        gate = jnp.dot(x, gate_up[:, here], preferred_element_type=jnp.float32)
        if first + tile <= kept:
            up = jnp.dot(x, gate_up[:, there], preferred_element_type=jnp.float32)
        else:
            there = pl.ds(units + first, kept - first)
            up = [
                jnp.dot(x, w, preferred_element_type=jnp.float32)
                for w in (gate_up[:, there], down[:, units:])
            ]
            up = jnp.concatenate(up, axis=1)
        gate, up = gate * gate_scale[:, here], up * up_scale[:, here]
        hidden.append((gate / (1.0 + jnp.exp(-gate)) * up).astype(jnp.bfloat16))
    hidden = jnp.concatenate(hidden, axis=1)
    for first in range(0, width, 512):
        here = pl.ds(first, 512)
        term = product(hidden, down[here, :units]).astype(jnp.bfloat16)
        out_near[:, here] = term[:half, :]
        out_far[:, here] = term[half:, :]


def mlp(near, far, gate_up, down_turned, gate_scale, up_scale):
    half, width = near.shape
    units = gate_scale.shape[0]
    return pl.pallas_call(
        mlp_kernel,
        in_specs=[VMEM] * 6,
        out_specs=[VMEM] * 2,
        out_shape=[jax.ShapeDtypeStruct((half, width), jnp.bfloat16)] * 2,
        compiler_params=KERNEL_PARAMS,
        cost_estimate=pl.CostEstimate(
            flops=12 * half * width * units,
            bytes_accessed=6 * width * units + 8 * half * width,
            transcendentals=2 * half * units,
        ),
    )(near, far, gate_up, down_turned, gate_scale[None], up_scale[None])


def mixer_kernel(
    place_ref, near_ref, far_ref, own_ref, below_ref, above_ref, beyond_ref, scale_ref,
    cosine_ref, sine_ref, within_ref, fading_ref, rising_ref, decay_ref, out_near_ref, out_far_ref,
    both, weight, query, key, value, mixed, sorted_,
):
    half = near_ref.shape[0]
    rows = half // 4
    core, y = place_ref[0], place_ref[1]

    def place_of(part, number):
        return pl.ds(pl.multiple_of(part * 2 * rows + number * rows, rows), rows)

    def whole_weight(k):
        for piece_ref, by in ((own_ref, 0), (below_ref, 3), (above_ref, 1), (beyond_ref, 2)):
            weight[k, :, lax.rem(y + by, 4), :, :] = piece_ref[:, k]
        return weight[k].reshape(-1, HEAD_DIM)

    for part in range(4):
        here = pl.ds(part * rows, rows)
        both[place_of(part, core), :] = near_ref[here, :]
        both[place_of(part, 1 - core), :] = far_ref[here, :]

    def projected(k):
        pre = jnp.dot(both[...], whole_weight(k), preferred_element_type=jnp.float32)
        return pre * scale_ref[:, k * HEAD_DIM : (k + 1) * HEAD_DIM]

    def turned(values):
        middle = HEAD_DIM // 2
        a, b = values[:, :middle], values[:, middle:]
        cosine, sine = cosine_ref[...], sine_ref[...]
        return jnp.concatenate([a * cosine - b * sine, b * cosine + a * sine], axis=1)

    query[...] = turned(projected(0)).astype(jnp.bfloat16)
    key[...] = turned(projected(1)).astype(jnp.bfloat16)
    value[...] = projected(2).astype(jnp.bfloat16)
    blocks = query.shape[0] // BLOCK
    state = None
    for n in range(blocks):
        place = pl.ds(n * BLOCK, BLOCK)
        q, k, v = query[place, :], key[place, :], value[place, :]
        weights = (product(q, k) * within_ref[...]).astype(jnp.bfloat16)
        combined = jnp.dot(weights, v, preferred_element_type=jnp.float32)
        if n > 0:
            queried = q.astype(jnp.float32) * rising_ref[...]
            combined += jnp.dot(
                queried, state, precision=HIGHEST, preferred_element_type=jnp.float32
            )
        if n < blocks - 1:
            faded = (k.astype(jnp.float32) * fading_ref[...]).T
            update = jnp.dot(
                faded,
                v.astype(jnp.float32),
                precision=HIGHEST,
                preferred_element_type=jnp.float32,
            )
            state = update if n == 0 else state * decay_ref[...] + update
        square = jnp.mean(combined * combined, axis=1, keepdims=True)
        normed = combined * lax.rsqrt(jnp.maximum(square, HEAD_FLOOR))
        mixed[place, :] = normed.astype(jnp.bfloat16)
    for part in range(4):
        here, there = pl.ds(part * rows, rows), pl.ds(half + part * rows, rows)
        sorted_[here, :] = mixed[place_of(part, core), :]
        sorted_[there, :] = mixed[place_of(part, 1 - core), :]
    output = whole_weight(3)
    for first in range(0, output.shape[0], 512):
        here = pl.ds(first, 512)
        term = product(sorted_[...], output[first : first + 512, :]).astype(jnp.bfloat16)
        out_near_ref[:, here] = term[:half, :]
        out_far_ref[:, here] = term[half:, :]


def mixer_tables(rows, rate):
    positions = jnp.arange(rows, dtype=jnp.float32)
    half = HEAD_DIM // 2
    frequency = ROTARY_BASE ** (-jnp.arange(half, dtype=jnp.float32) * 2.0 / HEAD_DIM)
    angles = positions[:, None] * frequency[None, :]
    inside = jnp.arange(BLOCK, dtype=jnp.float32)
    distance = inside[:, None] - inside[None, :]
    within = jnp.where(distance >= 0, jnp.exp(-rate * jnp.maximum(distance, 0.0)), 0.0)
    fading = jnp.exp(-rate * (BLOCK - 1.0 - inside[:, None])) * HEAD_DIM ** (-0.5)
    rising = jnp.exp(-rate * (inside[:, None] + 1.0))
    return (
        jnp.cos(angles),
        jnp.sin(angles),
        within * HEAD_DIM ** (-0.5),
        jnp.broadcast_to(fading, (BLOCK, HEAD_DIM)),
        jnp.broadcast_to(rising, (BLOCK, HEAD_DIM)),
        jnp.broadcast_to(jnp.exp(-rate * BLOCK), (1, HEAD_DIM)),
    )


def mixer(near, far, pieces, scales, tables, place):
    half_rows, width = near.shape
    rows = 2 * half_rows
    return pl.pallas_call(
        mixer_kernel,
        in_specs=[
            pl.BlockSpec(memory_space=pltpu.SMEM),
            *[VMEM] * (3 + len(pieces) + len(tables)),
        ],
        out_specs=[VMEM] * 2,
        out_shape=[jax.ShapeDtypeStruct((half_rows, width), jnp.bfloat16)] * 2,
        scratch_shapes=[
            pltpu.VMEM((rows, width), jnp.bfloat16),
            pltpu.VMEM((4, pieces[0].shape[0], 4, *pieces[0].shape[2:]), jnp.bfloat16),
            *[pltpu.VMEM((rows, HEAD_DIM), jnp.bfloat16) for _ in range(5)],
        ],
        compiler_params=KERNEL_PARAMS,
        cost_estimate=pl.CostEstimate(
            flops=10 * rows * width * HEAD_DIM,
            bytes_accessed=8 * width * HEAD_DIM + 4 * rows * width,
            transcendentals=rows,
        ),
    )(place, near, far, *pieces, scales[None], *tables)


def layer(
    residual_in,
    gain_first,
    gain_mixer,
    gain_second,
    gate_weight,
    gate_scale,
    up_weight,
    up_scale,
    down_weight,
    down_scale,
    query_weight,
    query_scale,
    key_weight,
    key_scale,
    value_weight,
    value_scale,
    output_weight,
    output_scale,
):
    low = jnp.bfloat16
    z, rows = lax.axis_size("z"), gate_weight.shape[0]
    hidden_width, local_width = down_weight.shape[0], query_weight.shape[1]
    first_width = 2 * hidden_width - MOVED
    packed, second_part, third_part = prepare(
        gate_weight, up_weight, down_weight, down_scale, query_weight, key_weight, value_weight,
        output_weight, output_scale,
    )
    packed_y = lax.all_to_all(packed, "y", 0, 0, tiled=True).reshape(-1, packed.shape[2])
    packed_y = lax.dynamic_update_slice(packed_y, third_part, (0, first_width))
    whole_z = lax.all_gather(packed_y, "z", axis=0, tiled=True)
    second_z = lax.all_gather(after(second_part, packed_y), "z", axis=0, tiled=True)
    second_near = y_neighbours(second_z)
    first_rows = collect_rows(after(residual_in, second_z), gain_first)
    second_far = y_opposite(*second_near)
    down_full = joined_over_y(
        *[
            x.reshape(1, z, rows, hidden_width + MOVED)
            for x in (second_z, *second_near, jnp.concatenate(second_far, axis=0))
        ]
    )[0]
    third_z = whole_z[:, first_width:]
    third_below = shifted(third_z, "y", 1)
    third_above = shifted(third_z, "y", -1)
    third_far = shifted(third_below, "y", 1)
    core = lax.axis_index("c")
    rate = head_rates(lax.axis_index("x") * lax.axis_size("c") + core, 1, TOK)[0]
    scales = jnp.concatenate([query_scale, key_scale, value_scale])
    place = jnp.stack([core, lax.axis_index("y")]).astype(jnp.int32)
    first_rows, scales, place = lax.optimization_barrier((first_rows, scales, place))
    first_term = mlp(*first_rows, whole_z, down_full, gate_scale, up_scale)
    tables = mixer_tables(TOK, rate)
    mlp_first = return_rows(*first_term)
    pieces = [
        x.reshape(-1, 4, rows, local_width)
        for x in (third_z, third_below, third_above, third_far)
    ]
    middle = (residual_in.astype(jnp.float32) + 0.5 * mlp_first).astype(low)
    mixer_rows = collect_rows(middle, gain_mixer)
    mixer_term = mixer(*mixer_rows, pieces, scales, tables, place)
    second = (middle.astype(jnp.float32) + return_rows(*mixer_term)).astype(low)
    second_rows = collect_rows(second, gain_second)
    mlp_second = return_rows(*mlp(*second_rows, whole_z, down_full, gate_scale, up_scale))
    return (second.astype(jnp.float32) + 0.5 * mlp_second).astype(low)


def solution(mesh):
    split = Mesh(mesh.devices.reshape(16, 4, 4, 2), FS_TP)
    in_specs = (
        P(FS_TP, None),
        P(),
        P(),
        P(),
        P(FS, TP),
        P(TP),
        P(FS, TP),
        P(TP),
        P(TP, FS),
        P(FS),
        P(FS, TP),
        P(TP),
        P(FS, TP),
        P(TP),
        P(FS, TP),
        P(TP),
        P(TP, FS),
        P(FS),
    )
    out_specs = P(FS_TP, None)
    return jax.shard_map(layer, mesh=split, in_specs=in_specs, out_specs=out_specs, check_vma=False)
```

```python
import jax
import jax.numpy as jnp
from jax import lax
from jax.experimental import pallas as pl
from jax.experimental.pallas import tpu as pltpu
from jax.sharding import Mesh
from jax.sharding import PartitionSpec as P


HEADS = 8
HEAD_DIM = 256
BLOCK = 64
TOK = 256
MOVED = 128
FS = ("z", "y")
TP = ("x", "c")
FS_TP = ("z", "y", "x", "c")


EPSILON = 1e-06
HEAD_FLOOR = 0.25
ROTARY_BASE = 10000.0
HIGHEST = lax.Precision.HIGHEST


def spread(own_rows):
    peers = lax.axis_size("x")
    sent = jnp.broadcast_to(own_rows[None], (peers, *own_rows.shape))
    return lax.all_to_all(sent, "x", 0, 0, tiled=True).reshape(-1, own_rows.shape[1])


def swapped(x):
    return lax.ppermute(x, "c", [(0, 1), (1, 0)])


def shifted(x, axis, by):
    peers = lax.axis_size(axis)
    return lax.ppermute(x, axis, [(i, (i + by) % peers) for i in range(peers)])


def after(x, first):
    return lax.optimization_barrier((x, first))[0]


def y_neighbours(part):
    return shifted(part, "y", 1), shifted(part, "y", -1)


def y_opposite(below, above):
    half = below.shape[0] // 2
    return shifted(below[:half], "y", 1), shifted(above[half:], "y", -1)


def joined_over_y(part, below, above, far):
    me, peers = lax.axis_index("y"), lax.axis_size("y")
    own = part[:, :, None]
    whole = jnp.broadcast_to(own, (*part.shape[:2], peers, *part.shape[2:]))
    for piece, by in ((below, 3), (far, 2), (above, 1)):
        place = (0, 0, (me + by) % peers, 0, 0)
        whole = lax.dynamic_update_slice(whole, piece[:, :, None], place)
    return whole.reshape(part.shape[0], -1, part.shape[3])


def prepare_kernel(
    gate_ref, up_ref, down_ref, down_scale_ref, query_ref, key_ref, value_ref, output_ref, output_scale_ref,
    first_ref, second_ref, third_ref,
):
    low = jnp.bfloat16
    rows, units = gate_ref.shape
    width = query_ref.shape[1]
    kept = units - MOVED
    for copy in range(first_ref.shape[0]):
        first_ref[copy, :, :units] = gate_ref[...].astype(low)
        first_ref[copy, :, units : units + kept] = up_ref[:, :kept].astype(low)
        first_ref[copy, :, units + kept :] = jnp.zeros((rows, width), low)
    second_ref[:, :units] = scaled_rows(down_ref[...], down_scale_ref[...])
    second_ref[:, units:] = up_ref[:, kept:].astype(low)
    for k, ref in enumerate((query_ref, key_ref, value_ref)):
        third_ref[pl.ds(k * rows, rows), :] = ref[...].astype(low)
    third_ref[pl.ds(3 * rows, rows), :] = scaled_rows(output_ref[...], output_scale_ref[...])


def scaled_rows(turned, factor):
    low = turned.astype(jnp.bfloat16).astype(jnp.float32)
    column = jnp.broadcast_to(factor, (8, factor.shape[1])).T[:, :1]
    return (low * column).astype(jnp.bfloat16)


def prepare(gate, up, down, down_scale, query, key, value, output, output_scale):
    rows, hidden_width = gate.shape
    width = query.shape[1]
    units = hidden_width
    first = (lax.axis_size("y"), rows, 2 * units - MOVED + width)
    shapes = (first, (rows, units + MOVED), (4 * rows, width))
    return pl.pallas_call(
        prepare_kernel,
        out_shape=[jax.ShapeDtypeStruct(x, jnp.bfloat16) for x in shapes],
        cost_estimate=pl.CostEstimate(
            flops=rows * (3 * hidden_width + 4 * width),
            bytes_accessed=6 * rows * (3 * hidden_width + 4 * width),
            transcendentals=0,
        ),
    )(
        gate, up, down.T, down_scale[None], query, key, value, output.T, output_scale[None]
    )


def normalize(sequence_rows, gain_vector):
    values = sequence_rows.astype(jnp.float32)
    scaled = values * lax.rsqrt(jnp.mean(values * values, axis=-1, keepdims=True) + EPSILON)
    return (scaled * gain_vector).astype(jnp.bfloat16)


def collect_rows(own_rows, gain_vector):
    near = spread(normalize(own_rows, gain_vector))
    return near, swapped(near)


def product(inputs, turned):
    return lax.dot_general(
        inputs, turned, (((1,), (1,)), ((), ())), preferred_element_type=jnp.float32
    )


def return_rows(near, far):
    pair = near.astype(jnp.float32) + swapped(far).astype(jnp.float32)
    pieces = pair.astype(jnp.bfloat16).reshape(lax.axis_size("x"), -1, near.shape[1])
    arrived = lax.all_to_all(pieces, "x", 0, 0, tiled=True)
    return arrived.astype(jnp.float32).sum(axis=0)


def head_rates(first_head, head_count, length):
    head_number = (first_head + jnp.arange(head_count)).astype(jnp.float32)
    return jnp.exp(jnp.log(1.0 / 16.0) + head_number / (HEADS - 1) * jnp.log(4.0 / length))


VMEM = pl.BlockSpec(memory_space=pltpu.VMEM)
KERNEL_PARAMS = pltpu.CompilerParams(vmem_limit_bytes=20 * 1024 * 1024)


def fetching_mlp_kernel(
    near_ref, far_ref, gate_up_ref, down_ref, gate_scale, up_scale, out_near, out_far, gate_up, down, arrived
):
    depth = gate_up.shape[0] // 4
    copies = [
        pltpu.make_async_copy(gate_up_ref.at[here, :], gate_up.at[here, :], arrived.at[k])
        for k, here in enumerate(pl.ds(k * depth, depth) for k in range(4))
    ]
    copies.append(pltpu.make_async_copy(down_ref, down, arrived.at[4]))
    for copy in copies:
        copy.start()
    for copy in copies:
        copy.wait()
    mlp_kernel(near_ref, far_ref, gate_up, down, gate_scale, up_scale, out_near, out_far)


def mlp_kernel(near_ref, far_ref, gate_up, down, gate_scale, up_scale, out_near, out_far):
    half, width = near_ref.shape
    units, tile = down.shape[1] - MOVED, 256
    kept = units - MOVED
    x = jnp.concatenate([near_ref[...], far_ref[...]], axis=0)
    hidden = []
    for first in range(0, units, tile):
        here, there = pl.ds(first, tile), pl.ds(units + first, tile)
        gate = jnp.dot(x, gate_up[:, here], preferred_element_type=jnp.float32)
        if first + tile <= kept:
            up = jnp.dot(x, gate_up[:, there], preferred_element_type=jnp.float32)
        else:
            there = pl.ds(units + first, kept - first)
            up = [
                jnp.dot(x, w, preferred_element_type=jnp.float32)
                for w in (gate_up[:, there], down[:, units:])
            ]
            up = jnp.concatenate(up, axis=1)
        gate, up = gate * gate_scale[:, here], up * up_scale[:, here]
        hidden.append((gate / (1.0 + jnp.exp(-gate)) * up).astype(jnp.bfloat16))
    hidden = jnp.concatenate(hidden, axis=1)
    for first in range(0, width, 512):
        here = pl.ds(first, 512)
        term = product(hidden, down[here, :units]).astype(jnp.bfloat16)
        out_near[:, here] = term[:half, :]
        out_far[:, here] = term[half:, :]


def mlp(near, far, gate_up, down_turned, gate_scale, up_scale, fetch=False):
    half, width = near.shape
    units = gate_scale.shape[0]
    weights, scratch, params = [VMEM] * 2, [], KERNEL_PARAMS
    if fetch:
        weights = [pl.BlockSpec(memory_space=pl.ANY)] * 2
        scratch = [pltpu.VMEM(x.shape, jnp.bfloat16) for x in (gate_up, down_turned)]
        scratch.append(pltpu.SemaphoreType.DMA((5,)))
        params = pltpu.CompilerParams(vmem_limit_bytes=60 * 1024 * 1024)
    return pl.pallas_call(
        fetching_mlp_kernel if fetch else mlp_kernel,
        in_specs=[VMEM] * 2 + weights + [VMEM] * 2,
        out_specs=[VMEM] * 2,
        out_shape=[jax.ShapeDtypeStruct((half, width), jnp.bfloat16)] * 2,
        scratch_shapes=scratch,
        compiler_params=params,
        cost_estimate=pl.CostEstimate(
            flops=12 * half * width * units,
            bytes_accessed=6 * width * units + 8 * half * width,
            transcendentals=2 * half * units,
        ),
    )(near, far, gate_up, down_turned, gate_scale[None], up_scale[None])


def mixer_kernel(
    place_ref, near_ref, far_ref, own_ref, below_ref, above_ref, beyond_ref, scale_ref,
    cosine_ref, sine_ref, within_ref, fading_ref, rising_ref, decay_ref, out_near_ref, out_far_ref,
    both, weight, query, key, value, mixed, sorted_,
):
    half = near_ref.shape[0]
    rows = half // 4
    core, y = place_ref[0], place_ref[1]

    def place_of(part, number):
        return pl.ds(pl.multiple_of(part * 2 * rows + number * rows, rows), rows)

    def whole_weight(k):
        for piece_ref, by in ((own_ref, 0), (below_ref, 3), (above_ref, 1), (beyond_ref, 2)):
            weight[k, :, lax.rem(y + by, 4), :, :] = piece_ref[:, k]
        return weight[k].reshape(-1, HEAD_DIM)

    for part in range(4):
        here = pl.ds(part * rows, rows)
        both[place_of(part, core), :] = near_ref[here, :]
        both[place_of(part, 1 - core), :] = far_ref[here, :]

    def projected(k):
        pre = jnp.dot(both[...], whole_weight(k), preferred_element_type=jnp.float32)
        return pre * scale_ref[:, k * HEAD_DIM : (k + 1) * HEAD_DIM]

    def turned(values):
        middle = HEAD_DIM // 2
        a, b = values[:, :middle], values[:, middle:]
        cosine, sine = cosine_ref[...], sine_ref[...]
        return jnp.concatenate([a * cosine - b * sine, b * cosine + a * sine], axis=1)

    query[...] = turned(projected(0)).astype(jnp.bfloat16)
    key[...] = turned(projected(1)).astype(jnp.bfloat16)
    value[...] = projected(2).astype(jnp.bfloat16)
    blocks = query.shape[0] // BLOCK
    state = None
    for n in range(blocks):
        place = pl.ds(n * BLOCK, BLOCK)
        q, k, v = query[place, :], key[place, :], value[place, :]
        weights = (product(q, k) * within_ref[...]).astype(jnp.bfloat16)
        combined = jnp.dot(weights, v, preferred_element_type=jnp.float32)
        if n > 0:
            queried = q.astype(jnp.float32) * rising_ref[...]
            combined += jnp.dot(
                queried, state, precision=HIGHEST, preferred_element_type=jnp.float32
            )
        if n < blocks - 1:
            faded = (k.astype(jnp.float32) * fading_ref[...]).T
            update = jnp.dot(
                faded,
                v.astype(jnp.float32),
                precision=HIGHEST,
                preferred_element_type=jnp.float32,
            )
            state = update if n == 0 else state * decay_ref[...] + update
        square = jnp.mean(combined * combined, axis=1, keepdims=True)
        normed = combined * lax.rsqrt(jnp.maximum(square, HEAD_FLOOR))
        mixed[place, :] = normed.astype(jnp.bfloat16)
    for part in range(4):
        here, there = pl.ds(part * rows, rows), pl.ds(half + part * rows, rows)
        sorted_[here, :] = mixed[place_of(part, core), :]
        sorted_[there, :] = mixed[place_of(part, 1 - core), :]
    output = whole_weight(3)
    for first in range(0, output.shape[0], 512):
        here = pl.ds(first, 512)
        term = product(sorted_[...], output[first : first + 512, :]).astype(jnp.bfloat16)
        out_near_ref[:, here] = term[:half, :]
        out_far_ref[:, here] = term[half:, :]


def mixer_tables(rows, rate):
    positions = jnp.arange(rows, dtype=jnp.float32)
    half = HEAD_DIM // 2
    frequency = ROTARY_BASE ** (-jnp.arange(half, dtype=jnp.float32) * 2.0 / HEAD_DIM)
    angles = positions[:, None] * frequency[None, :]
    inside = jnp.arange(BLOCK, dtype=jnp.float32)
    distance = inside[:, None] - inside[None, :]
    within = jnp.where(distance >= 0, jnp.exp(-rate * jnp.maximum(distance, 0.0)), 0.0)
    fading = jnp.exp(-rate * (BLOCK - 1.0 - inside[:, None])) * HEAD_DIM ** (-0.5)
    rising = jnp.exp(-rate * (inside[:, None] + 1.0))
    return (
        jnp.cos(angles),
        jnp.sin(angles),
        within * HEAD_DIM ** (-0.5),
        jnp.broadcast_to(fading, (BLOCK, HEAD_DIM)),
        jnp.broadcast_to(rising, (BLOCK, HEAD_DIM)),
        jnp.broadcast_to(jnp.exp(-rate * BLOCK), (1, HEAD_DIM)),
    )


def mixer(near, far, pieces, scales, tables, place):
    half_rows, width = near.shape
    rows = 2 * half_rows
    return pl.pallas_call(
        mixer_kernel,
        in_specs=[
            pl.BlockSpec(memory_space=pltpu.SMEM),
            *[VMEM] * (3 + len(pieces) + len(tables)),
        ],
        out_specs=[VMEM] * 2,
        out_shape=[jax.ShapeDtypeStruct((half_rows, width), jnp.bfloat16)] * 2,
        scratch_shapes=[
            pltpu.VMEM((rows, width), jnp.bfloat16),
            pltpu.VMEM((4, pieces[0].shape[0], 4, *pieces[0].shape[2:]), jnp.bfloat16),
            *[pltpu.VMEM((rows, HEAD_DIM), jnp.bfloat16) for _ in range(5)],
        ],
        compiler_params=KERNEL_PARAMS,
        cost_estimate=pl.CostEstimate(
            flops=10 * rows * width * HEAD_DIM,
            bytes_accessed=8 * width * HEAD_DIM + 4 * rows * width,
            transcendentals=rows,
        ),
    )(place, near, far, *pieces, scales[None], *tables)


def layer(
    residual_in,
    gain_first,
    gain_mixer,
    gain_second,
    gate_weight,
    gate_scale,
    up_weight,
    up_scale,
    down_weight,
    down_scale,
    query_weight,
    query_scale,
    key_weight,
    key_scale,
    value_weight,
    value_scale,
    output_weight,
    output_scale,
):
    low = jnp.bfloat16
    z, rows = lax.axis_size("z"), gate_weight.shape[0]
    hidden_width, local_width = down_weight.shape[0], query_weight.shape[1]
    first_width = 2 * hidden_width - MOVED
    packed, second_part, third_part = prepare(
        gate_weight, up_weight, down_weight, down_scale, query_weight, key_weight, value_weight,
        output_weight, output_scale,
    )
    packed_y = lax.all_to_all(packed, "y", 0, 0, tiled=True).reshape(-1, packed.shape[2])
    packed_y = lax.dynamic_update_slice(packed_y, third_part, (0, first_width))
    whole_z = lax.all_gather(packed_y, "z", axis=0, tiled=True)
    second_z = lax.all_gather(after(second_part, packed_y), "z", axis=0, tiled=True)
    second_near = y_neighbours(second_z)
    first_rows = collect_rows(after(residual_in, second_z), gain_first)
    second_far = y_opposite(*second_near)
    down_full = joined_over_y(
        *[
            x.reshape(1, z, rows, hidden_width + MOVED)
            for x in (second_z, *second_near, jnp.concatenate(second_far, axis=0))
        ]
    )[0]
    third_z = whole_z[:, first_width:]
    third_below = shifted(third_z, "y", 1)
    third_above = shifted(third_z, "y", -1)
    third_far = shifted(third_below, "y", 1)
    core = lax.axis_index("c")
    rate = head_rates(lax.axis_index("x") * lax.axis_size("c") + core, 1, TOK)[0]
    scales = jnp.concatenate([query_scale, key_scale, value_scale])
    place = jnp.stack([core, lax.axis_index("y")]).astype(jnp.int32)
    first_rows, scales, place = lax.optimization_barrier((first_rows, scales, place))
    first_term = mlp(*first_rows, whole_z, down_full, gate_scale, up_scale, fetch=True)
    tables = mixer_tables(TOK, rate)
    mlp_first = return_rows(*first_term)
    pieces = [
        x.reshape(-1, 4, rows, local_width)
        for x in (third_z, third_below, third_above, third_far)
    ]
    middle = (residual_in.astype(jnp.float32) + 0.5 * mlp_first).astype(low)
    mixer_rows = collect_rows(middle, gain_mixer)
    mixer_term = mixer(*mixer_rows, pieces, scales, tables, place)
    second = (middle.astype(jnp.float32) + return_rows(*mixer_term)).astype(low)
    second_rows = collect_rows(second, gain_second)
    mlp_second = return_rows(*mlp(*second_rows, whole_z, down_full, gate_scale, up_scale))
    return (second.astype(jnp.float32) + 0.5 * mlp_second).astype(low)


def solution(mesh):
    split = Mesh(mesh.devices.reshape(16, 4, 4, 2), FS_TP)
    in_specs = (
        P(FS_TP, None),
        P(),
        P(),
        P(),
        P(FS, TP),
        P(TP),
        P(FS, TP),
        P(TP),
        P(TP, FS),
        P(FS),
        P(FS, TP),
        P(TP),
        P(FS, TP),
        P(TP),
        P(FS, TP),
        P(TP),
        P(TP, FS),
        P(FS),
    )
    out_specs = P(FS_TP, None)
    return jax.shard_map(layer, mesh=split, in_specs=in_specs, out_specs=out_specs, check_vma=False)
```
